32 devices in a mesh: sp: 4 (over z), fs: 4 (over y, x), tp: 2 (over core).
Axes of the slice: x: 2, y: 2, z: 4, core: 2. Of those that a mesh axis runs over, the one named last changes fastest.
Arguments:
- tokens: bfloat16 [4, 512, 2048], P('fs', ('sp', 'tp')), may hold values from -6 to 6
- input_norm_gain: float32 [2048], replicated, may hold values from 0.1 to 1.9
- pooling_input_weight: bfloat16 [2048, 1024], P('sp', 'tp'), may hold values from -0.125 to 0.125
- query_weight: bfloat16 [2048, 1024], P('sp', 'tp'), may hold values from -0.125 to 0.125
- forget_weight: bfloat16 [2048, 1024], P('sp', 'tp'), may hold values from -0.125 to 0.125
- value_weight: bfloat16 [2048, 1024], P('sp', 'tp'), may hold values from -0.125 to 0.125
- pooling_group_maps: bfloat16 [4, 256, 256], P('tp'), may hold values from -0.375 to 0.375
- pooling_scale: float32 [1024], P('tp'), may hold values from 0.1 to 1.9
- lower_bound_logits: float32 [1024], P('tp')
- decay_spike: float32 [4, 512, 8], P('fs', 'sp', 'tp'), may hold values from -0.75 to 0
- head_norm_gain: float32 [1024], P('tp'), may hold values from 0.1 to 1.9
- pooling_output_weight: bfloat16 [1024, 2048], P('tp', 'sp'), may hold values from -0.125 to 0.125
- recurrent_output_weight: bfloat16 [1024, 2048], P('tp', 'sp'), may hold values from -0.125 to 0.125
Outputs:
- mixed: bfloat16 [4, 512, 2048], P('fs', ('sp', 'tp'))
The draws below stay inside these ranges and needn't reach their ends.
All inputs are finite; a program needn't handle non-finite values.
Results may differ from the reference program's by a relative error of at most 0.013.
Values may be sent and summed in bfloat16 or wider, within the bound.
No kernel may reach another device: no remote copies, remote signals or barrier semaphores. Data moves between devices by JAX's collectives and lax.ppermute only.
A program may use at most 64 MiB of HBM per device.

```python
import jax
import jax.numpy as jnp
from jax import lax

D = 2048
POOL_GROUP = 256
POOL_GROUPS = 4
HEAD = 128
RECURRENT_HEADS = 8
BLOCK = 64
TOK_DEV = 128
D_POOL = 1024
D_REC = 1024
LEN = 512
SEQUENCE_COUNT = 4
N_TP = 2


def head_kinds(key):
    ranking = jax.random.permutation(jax.random.fold_in(key, 11), RECURRENT_HEADS)
    return ranking < RECURRENT_HEADS // 2


def draw_lower_bound_logits(key, part):
    lasting = head_kinds(key)
    spread = jax.random.uniform(jax.random.fold_in(key, 12), (RECURRENT_HEADS, HEAD), jnp.float32)
    slow_rate = 0.3 * jnp.exp(jnp.log(4.0) * spread) / LEN
    fast_rate = 0.03 * jnp.exp(jnp.log(10.0 / 3.0) * spread)
    chosen = jnp.where(lasting[:, None], slow_rate, fast_rate)
    return (jnp.log1p(-chosen) - jnp.log(chosen)).reshape(D_REC)


def draw_decay_spike(key, part):
    lasting = head_kinds(key)
    devices = LEN // TOK_DEV
    spread = jax.random.uniform(jax.random.fold_in(key, 21), (SEQUENCE_COUNT, devices, RECURRENT_HEADS), jnp.float32)
    fast_rate = 0.004 * jnp.exp(jnp.log(5.0) * spread)
    slow_rate = 0.1 * jnp.exp(jnp.log(6.0) * spread) / LEN
    local_decay_rate = jnp.repeat(jnp.where(lasting[None, None, :], slow_rate, fast_rate), TOK_DEV, axis=1)
    third_length = LEN // 3
    spike_locations = jax.random.randint(jax.random.fold_in(key, 22), (SEQUENCE_COUNT, 3, RECURRENT_HEADS), 0, third_length)
    spike_locations = spike_locations + third_length * jnp.arange(3, dtype=jnp.int32)[None, :, None]
    kept_fraction = jax.random.uniform(jax.random.fold_in(key, 23), (SEQUENCE_COUNT, 3, RECURRENT_HEADS), jnp.float32, 0.55, 0.8)
    position_index = jnp.arange(LEN, dtype=jnp.int32)
    agreement = (position_index[None, :, None, None] == spike_locations[:, None, :, :]).astype(jnp.float32)
    spikes = jnp.sum(agreement * jnp.log(kept_fraction)[:, None, :, :], axis=2)
    return spikes - local_decay_rate


def shard_levels(own_key, shape, split, smallest, largest):
    level, own = 1.0, jax.random.fold_in(own_key, 6)
    for axis_at, blocks in split:
        steps = jnp.exp(jax.random.uniform(jax.random.fold_in(own, axis_at), (blocks,), jnp.float32, smallest / len(split), largest / len(split)))
        level = level * jnp.repeat(steps, shape[axis_at] // blocks).reshape([-1 if axis == axis_at else 1 for axis in range(len(shape))])
    return level


def scatter_about(rng, dims, scale, bound, shards=(), kind=jnp.bfloat16):
    drawn = jax.random.normal(rng, dims, jnp.float32) * scale
    if len(shards) > 0:
        drawn = shard_levels(rng, dims, shards, -0.22, 0.18) * drawn
    return jnp.clip(drawn, min=-bound, max=bound).astype(kind)


def setup_inputs(seed: int = 0) -> dict:
    seeds = jax.random.split(jax.random.key(seed), 14)
    return {
        "tokens": scatter_about(seeds[0], (SEQUENCE_COUNT, LEN, D), 1.0, 6.0, ((0, 4), (1, 8))),
        "input_norm_gain": jnp.clip(1.0 + 0.18 * jax.random.normal(seeds[1], (D,), jnp.float32), 0.1, 1.9),
        "pooling_input_weight": scatter_about(seeds[2], (D, D_POOL), D ** -0.5, 0.125, ((0, 4), (1, 2))),
        "query_weight": scatter_about(seeds[3], (D, D_REC), D ** -0.5, 0.125, ((0, 4), (1, 2))),
        "forget_weight": scatter_about(seeds[4], (D, D_REC), D ** -0.5, 0.125, ((0, 4), (1, 2))),
        "value_weight": scatter_about(seeds[5], (D, D_REC), D ** -0.5, 0.125, ((0, 4), (1, 2))),
        "pooling_group_maps": scatter_about(seeds[6], (POOL_GROUPS, POOL_GROUP, POOL_GROUP), POOL_GROUP ** -0.5, 0.375, ((0, 2),)),
        "pooling_scale": jnp.clip(1.0 + 0.18 * jax.random.normal(seeds[7], (D_POOL,), jnp.float32), 0.1, 1.9),
        "lower_bound_logits": draw_lower_bound_logits(jax.random.fold_in(seeds[13], 71), 0),
        "decay_spike": draw_decay_spike(jax.random.fold_in(seeds[13], 71), 0),
        "head_norm_gain": jnp.clip(1.0 + 0.18 * jax.random.normal(seeds[10], (D_REC,), jnp.float32), 0.1, 1.9),
        "pooling_output_weight": scatter_about(seeds[11], (D_POOL, D), (D_POOL + D_REC) ** -0.5, 0.125, ((0, 2), (1, 4))),
        "recurrent_output_weight": scatter_about(seeds[12], (D_REC, D), (D_POOL + D_REC) ** -0.5, 0.125, ((0, 2), (1, 4))),
    }


EPSILON = 1e-06
HIGHEST = lax.Precision.HIGHEST

def stored(values):
    return lax.optimization_barrier(values.astype(jnp.bfloat16))

def rms_scale(values, gain):
    return values * lax.rsqrt(lax.optimization_barrier(jnp.mean(values * values, axis=-1, keepdims=True)) + EPSILON) * gain

def pooling(pool_input, pooling_group_maps, pooling_scale):
    length_total = pool_input.shape[0]
    groups = pooling_group_maps.shape[0]
    group_size = pooling_group_maps.shape[1]
    reach_rows = 2 ** groups
    padded = jnp.pad(pool_input.astype(jnp.float32).reshape(length_total, groups, group_size), ((reach_rows, 0), (0, 0), (0, 0)))
    windows = 2 ** (jnp.arange(groups, dtype=jnp.int32) + 1)
    window_sum = jnp.zeros((length_total, groups, group_size), jnp.float32)
    for offset in range(reach_rows):
        inside = (offset < windows).astype(jnp.float32)
        window_sum = window_sum + padded[reach_rows - offset:reach_rows - offset + length_total] * inside[:, None]
    counts = jnp.minimum(jnp.arange(length_total, dtype=jnp.int32)[:, None] + 1, windows[None, :]).astype(jnp.float32)
    pool_diff = stored(window_sum / counts[:, :, None] - padded[reach_rows:])
    mapped = jnp.einsum('tgc,gcd->tgd', pool_diff.astype(jnp.float32), pooling_group_maps.astype(jnp.float32))
    return (mapped.reshape(length_total, groups * group_size) * pooling_scale).astype(jnp.bfloat16)

def linear_recurrence(query_matrix, forget_gate_logit, value_projected, lower_bound_logits, spike_row, head_norm_gain):
    length_total, width = query_matrix.shape
    number_heads = spike_row.shape[1]
    head_width = width // number_heads
    block_layout = (length_total // BLOCK, BLOCK, number_heads, head_width)
    reader = jax.nn.silu(query_matrix.astype(jnp.float32)).reshape(block_layout)
    key_gate_value = jax.nn.sigmoid(-lower_bound_logits) * jax.nn.sigmoid(-forget_gate_logit.astype(jnp.float32))
    decay_logarithm = (jnp.log1p(-key_gate_value).reshape(length_total, number_heads, head_width) + spike_row[:, :, None]).reshape(block_layout)
    key_rows = key_gate_value.reshape(block_layout)
    value_rows = value_projected.astype(jnp.float32).reshape(block_layout)
    causal = (jnp.arange(BLOCK)[:, None] >= jnp.arange(BLOCK)[None, :]).astype(jnp.float32)

    def advance(carried, input_batch):
        block_reader, block_key, block_value, block_log = input_batch
        inner_log = jnp.cumsum(block_log, axis=0)
        read_scaled = block_reader * jnp.exp(inner_log)
        key_scaled = block_key * jnp.exp(-inner_log)
        scores = jnp.einsum('thd,shd->hts', read_scaled, key_scaled, precision=HIGHEST) * causal
        output = jnp.einsum('hts,she->the', scores, block_value, precision=HIGHEST)
        output = output + jnp.einsum('thd,hde->the', read_scaled, carried, precision=HIGHEST)
        closing = inner_log[-1]
        key_tail = block_key * jnp.exp(closing[None] - inner_log)
        carried = jnp.exp(closing)[:, :, None] * carried + jnp.einsum('shd,she->hde', key_tail, block_value, precision=HIGHEST)
        return (carried, output)
    initial = jnp.zeros((number_heads, head_width, head_width), jnp.float32)
    final_state, read_out = lax.scan(advance, initial, (reader, key_rows, value_rows, decay_logarithm))
    read_out = read_out.reshape(length_total, number_heads, head_width)
    return (rms_scale(read_out, 1.0).reshape(length_total, width) * head_norm_gain).astype(jnp.bfloat16)

def reference(tokens, input_norm_gain, pooling_input_weight, query_weight, forget_weight, value_weight, pooling_group_maps, pooling_scale, lower_bound_logits, decay_spike, head_norm_gain, pooling_output_weight, recurrent_output_weight):
    pool_width = pooling_input_weight.shape[1] // N_TP
    rec_width = query_weight.shape[1] // N_TP

    def sequence_tokens(input_batch):
        token_series, spike_row = input_batch
        normed = rms_scale(token_series.astype(jnp.float32), input_norm_gain).astype(jnp.bfloat16)
        pool_input = stored(jnp.dot(normed, pooling_input_weight, preferred_element_type=jnp.float32))
        query_matrix = stored(jnp.dot(normed, query_weight, preferred_element_type=jnp.float32))
        forget_gate_logit = stored(jnp.dot(normed, forget_weight, preferred_element_type=jnp.float32))
        value_projected = stored(jnp.dot(normed, value_weight, preferred_element_type=jnp.float32))
        pool_out = pooling(pool_input, pooling_group_maps, pooling_scale)
        recurrent_output = linear_recurrence(query_matrix, forget_gate_logit, value_projected, lower_bound_logits, spike_row, head_norm_gain)
        mixed_sum = jnp.zeros((token_series.shape[0], pooling_output_weight.shape[1]), jnp.float32)
        for member in range(N_TP):
            pool_lo = member * pool_width
            rec_lo = member * rec_width
            partial_value = jnp.dot(pool_out[:, pool_lo:pool_lo + pool_width], pooling_output_weight[pool_lo:pool_lo + pool_width], preferred_element_type=jnp.float32)
            partial_value = partial_value + jnp.dot(recurrent_output[:, rec_lo:rec_lo + rec_width], recurrent_output_weight[rec_lo:rec_lo + rec_width], preferred_element_type=jnp.float32)
            mixed_sum = mixed_sum + stored(partial_value).astype(jnp.float32)
        return mixed_sum.astype(jnp.bfloat16)
    return lax.map(sequence_tokens, (tokens, decay_spike))
```

```python
import jax
import jax.numpy as jnp
from jax import lax
from jax.sharding import PartitionSpec as P

BLOCK = 64


EPSILON = 1e-06
HIGHEST = lax.Precision.HIGHEST


def shifted(value, axis, steps):
    count = lax.axis_size(axis)
    first, last = (max(0, -steps), min(count, count - steps))
    return lax.ppermute(value, axis, [(source, source + steps) for source in range(first, last)])


def entering(shard, axis, join, neutral):
    place = lax.axis_index(axis)
    gathered = jax.tree.map(
        lambda a, kind: lax.all_gather(a.astype(kind), axis), shard, (jnp.bfloat16, jnp.bfloat16)
    )
    state = jax.tree.map(lambda a, e: jnp.zeros_like(a) + jnp.asarray(e, a.dtype), shard, neutral)

    def one(step, state):
        return join(
            state,
            jax.tree.map(
                lambda a, own: lax.dynamic_index_in_dim(a, step, 0, False).astype(own.dtype),
                gathered,
                shard,
            ),
        )

    return lax.fori_loop(0, place, one, state)


def rms_scale(values, gain):
    return values * lax.rsqrt(jnp.mean(values * values, axis=-1, keepdims=True) + EPSILON) * gain


def join_state(earlier, later):
    decay_one, state_one = earlier
    decay_two, state_two = later
    return (decay_one * decay_two, decay_two[..., None] * state_one + state_two)


def swapped(value, axis, bits):
    count = lax.axis_size(axis)
    return lax.ppermute(value, axis, [(source, source ^ bits) for source in range(count)])


def turned(value, axis, steps):
    count = lax.axis_size(axis)
    return lax.ppermute(value, axis, [(source, (source + steps) % count) for source in range(count)])


def picked(stack, place):
    return lax.dynamic_index_in_dim(stack, place, 0, False)


def heads_divide(tokens, query_weight, pooling_input_weight, pooling_group_maps, decay_spike, out_weight):
    planes, members, cores = (lax.axis_size(axis) for axis in ("sp", "fs", "tp"))
    heads = decay_spike.shape[2]
    head_width = query_weight.shape[1] // heads
    return (
        cores == 2
        and members & (members - 1) == 0
        and heads == planes
        and pooling_group_maps.shape[0] * cores == heads
        and pooling_input_weight.shape[1] == query_weight.shape[1]
        and tokens.shape[0] == 1
        and decay_spike.shape[1] == cores * tokens.shape[1]
        and query_weight.shape[0] % members == 0
        and out_weight.shape[1] == members * head_width
        and (planes * decay_spike.shape[1]) % BLOCK == 0
    )


def by_heads(
    tokens,
    input_norm_gain,
    pooling_input_weight,
    query_weight,
    forget_weight,
    value_weight,
    pooling_group_maps,
    pooling_scale,
    lower_bound_logits,
    decay_spike,
    head_norm_gain,
    pooling_output_weight,
    recurrent_output_weight,
):
    planes, members, cores = (lax.axis_size(axis) for axis in ("sp", "fs", "tp"))
    plane, member, core = (lax.axis_index(axis) for axis in ("sp", "fs", "tp"))
    heads = decay_spike.shape[2]
    head = cores * plane + core
    column = head % heads
    partner_column = (cores * plane + 1 - core) % heads
    owns = head // heads == core
    rows_local, width_local = query_weight.shape
    width = width_local // heads
    row_slice = rows_local // members
    features = tokens.shape[2]
    inputs = (pooling_input_weight, query_weight, forget_weight, value_weight)
    outputs = (pooling_output_weight, recurrent_output_weight)
    count_in = len(inputs) * row_slice

    def packed(place, part):
        return jnp.concatenate(
            [
                lax.dynamic_slice(w, (part * row_slice, place * width), (row_slice, width))
                for w in inputs
            ]
            + [
                lax.dynamic_slice(w, (place * width, part * width), (width, width))
                for w in outputs
            ],
            axis=0,
        )

    arrived = []
    for step in range(planes):
        pairs = [
            (p * cores + c, heads * c + (p + step) % heads)
            for p in range(planes)
            for c in range(cores)
        ]
        arrived.append(
            lax.ppermute(packed((plane + step) % heads, member), ("sp", "tp"), pairs)
        )
    group_local = plane % pooling_group_maps.shape[0]
    group_map = picked(pooling_group_maps, group_local)

    def own_block(place, side):
        return jnp.concatenate(
            [packed(place, part) for part in range(members)]
            + [lax.dynamic_slice_in_dim(group_map, side * width, width, 1)],
            axis=0,
        )

    def own_vectors(place):
        return jnp.stack(
            [
                lax.dynamic_slice_in_dim(v, place * width, width, 0)
                for v in (pooling_scale, lower_bound_logits, head_norm_gain)
            ]
        )

    block_rows = count_in + len(outputs) * width
    block = jnp.where(
        owns, own_block(column, core), swapped(own_block(partner_column, 1 - core), "tp", 1)
    )
    vectors = jnp.where(
        owns, own_vectors(column), swapped(own_vectors(partner_column), "tp", 1)
    )
    map_columns = block[members * block_rows :]
    own_parts = block[: members * block_rows].reshape(members, block_rows, width)

    normed = rms_scale(tokens[0].astype(jnp.float32), input_norm_gain).astype(jnp.bfloat16)
    spikes = decay_spike[0].T
    spikes_high = lax.reduce_precision(spikes, 8, 7)
    spike_rows = jnp.concatenate([spikes_high, spikes - spikes_high], axis=0).astype(jnp.bfloat16)
    message = jnp.concatenate(
        [normed, jnp.pad(spike_rows, ((0, 0), (0, features - spike_rows.shape[1])))], axis=0
    )
    own_rows = [message] + [turned(message, "sp", step) for step in range(1, planes)]
    partner_rows = [swapped(rows, "tp", 1) for rows in own_rows]
    rows_each = normed.shape[0]

    gathered = jnp.stack(arrived)
    others = jnp.stack(
        [picked(gathered, (column - plane - k) % planes) for k in range(1, planes)]
    )
    shared = jnp.stack([others] + [swapped(others, "fs", bits) for bits in range(1, members)])
    by_member = jnp.stack([picked(shared, member ^ part) for part in range(members)])
    by_offset = jnp.concatenate([own_parts[:, None], by_member], axis=1)
    weights = jnp.stack(
        [
            lax.dynamic_index_in_dim(by_offset, (p - plane) % planes, 1, False)
            for p in range(planes)
        ]
    )
    weights_in = weights[:, :, :count_in].reshape(planes, members, len(inputs), row_slice, width)
    weights_in = jnp.moveaxis(weights_in, 2, 3).reshape(features, len(inputs) * width)
    weights_out = weights[:, :, count_in:].reshape(planes, members, len(outputs), width, width)
    weights_out = jnp.moveaxis(weights_out, (2, 3), (0, 1)).reshape(
        len(outputs) * width, planes * members * width
    )

    both = jnp.stack([jnp.stack(own_rows), jnp.stack(partner_rows)])
    ordered = jnp.stack([picked(both, core ^ side) for side in range(cores)])
    ordered = jnp.stack(
        [
            lax.dynamic_index_in_dim(ordered, (plane - p) % planes, 1, False)
            for p in range(planes)
        ]
    )
    all_tokens = ordered[:, :, :rows_each].reshape(-1, features)
    length = all_tokens.shape[0]
    spike_parts = picked(jnp.moveaxis(ordered, 1, 0), head // heads)[
        :, rows_each:, : spikes.shape[1]
    ]
    spike_parts = spike_parts.astype(jnp.float32)
    spike_all = spike_parts[:, :heads] + spike_parts[:, heads:]
    spike = lax.dynamic_index_in_dim(spike_all, column, 1, False).reshape(length)

    projected = jnp.dot(all_tokens, weights_in, preferred_element_type=jnp.float32)
    projected = projected.astype(jnp.bfloat16)
    pool_input, query, forget_logit, value = (
        projected[:, n * width : (n + 1) * width].astype(jnp.float32) for n in range(len(inputs))
    )
    pool_scale, lower_bound, head_gain = vectors

    window = jnp.left_shift(jnp.int32(2), plane)
    window_sum = pool_input
    chosen = jnp.zeros_like(pool_input)
    for group in range(planes):
        reach = 2**group
        window_sum = window_sum + jnp.pad(window_sum, ((reach, 0), (0, 0)))[:length]
        chosen = jnp.where(plane == group, window_sum, chosen)
    counts = jnp.minimum(jnp.arange(length, dtype=jnp.int32) + 1, window).astype(jnp.float32)
    pool_diff = (chosen / counts[:, None] - pool_input).astype(jnp.bfloat16)
    pool_other = swapped(pool_diff, "tp", 1)
    pool_both = jnp.where(
        core == 0,
        jnp.concatenate([pool_diff, pool_other], axis=1),
        jnp.concatenate([pool_other, pool_diff], axis=1),
    )
    pool_out = jnp.dot(pool_both, map_columns, preferred_element_type=jnp.float32) * pool_scale
    pool_out = pool_out.astype(jnp.bfloat16)

    blocks = length // BLOCK
    layout = (blocks, BLOCK, width)
    reader = jax.nn.silu(query).reshape(layout)
    key_gate = jax.nn.sigmoid(-lower_bound) * jax.nn.sigmoid(-forget_logit)
    log_decay = (jnp.log1p(-key_gate) + spike[:, None]).reshape(layout)
    key_rows = key_gate.reshape(layout)
    value_rows = value.reshape(layout)
    inner_log = jnp.cumsum(log_decay, axis=1)
    read_scaled = reader * jnp.exp(inner_log)
    key_scaled = key_rows * jnp.exp(-inner_log)
    causal = (jnp.arange(BLOCK)[:, None] >= jnp.arange(BLOCK)[None, :]).astype(jnp.float32)
    scores = jnp.einsum("ntd,nsd->nts", read_scaled, key_scaled, precision=HIGHEST) * causal
    within = jnp.einsum("nts,nse->nte", scores, value_rows, precision=HIGHEST)
    closing = inner_log[:, -1]
    key_tail = key_rows * jnp.exp(closing[:, None] - inner_log)
    deltas = jnp.einsum("nsd,nse->nde", key_tail, value_rows, precision=HIGHEST)
    block_decay = jnp.exp(closing)
    state = jnp.zeros((width, width), jnp.float32)
    entry_states = []
    for n in range(blocks):
        entry_states.append(state)
        state = block_decay[n][:, None] * state + deltas[n]
    start_states = jnp.stack(entry_states)
    read_out = within + jnp.einsum("ntd,nde->nte", read_scaled, start_states, precision=HIGHEST)
    rec_out = (rms_scale(read_out, 1.0) * head_gain).astype(jnp.bfloat16).reshape(length, width)

    mixed = jnp.concatenate([pool_out, rec_out], axis=1).reshape(planes, cores, rows_each, -1)

    def partial_rows(side):
        part = lax.dynamic_index_in_dim(mixed, side, 1, False)
        return jnp.einsum("prc,cd->prd", part, weights_out, preferred_element_type=jnp.float32)

    from_partner = swapped(partial_rows(1 - core).astype(jnp.bfloat16), "tp", 1)
    plane_sums = partial_rows(core) + from_partner.astype(jnp.float32)
    total = picked(plane_sums, plane)
    for step in range(1, planes):
        sent = picked(plane_sums, (plane + step) % planes).astype(jnp.bfloat16)
        total = total + turned(sent, "sp", step).astype(jnp.float32)
    return total.astype(jnp.bfloat16)[None]


def body(*arrays):
    tokens, _, pool_in, query_in, _, _, maps, _, _, spike, _, pool_out, _ = arrays
    if heads_divide(tokens, query_in, pool_in, maps, spike, pool_out):
        return by_heads(*arrays)
    return by_positions(*arrays)


def by_positions(
    tokens,
    input_norm_gain,
    pooling_input_weight,
    query_weight,
    forget_weight,
    value_weight,
    pooling_group_maps,
    pooling_scale,
    lower_bound_logits,
    decay_spike,
    head_norm_gain,
    pooling_output_weight,
    recurrent_output_weight,
):
    gathered = lax.all_gather(tokens, "tp", axis=1, tiled=True)[0]
    length_total = gathered.shape[0]
    normed = rms_scale(gathered.astype(jnp.float32), input_norm_gain).astype(jnp.bfloat16)
    pool_width = pooling_input_weight.shape[1]
    rec_width = query_weight.shape[1]
    stacked = jnp.concatenate(
        [pooling_input_weight, query_weight, forget_weight, value_weight], axis=1
    )
    out_local = jnp.concatenate([pooling_output_weight, recurrent_output_weight], axis=0)
    groups_fs = lax.axis_size("fs")
    member = lax.axis_index("fs")
    slice_width = stacked.shape[1] // groups_fs
    own_slice = lax.dynamic_slice_in_dim(stacked, member * slice_width, slice_width, 1)
    column_part = lax.all_gather(own_slice, "sp", axis=0, tiled=True)
    full_input = lax.all_gather(column_part, "fs", axis=1, tiled=True)
    projected = jnp.dot(normed, full_input, preferred_element_type=jnp.float32)
    slice_height = out_local.shape[0] // groups_fs
    own_rows = lax.dynamic_slice_in_dim(out_local, member * slice_height, slice_height, 0)
    row_part = lax.all_gather(own_rows, "sp", axis=1, tiled=True)
    out_full = lax.all_gather(row_part, "fs", axis=0, tiled=True)
    rounded = lax.optimization_barrier(projected.astype(jnp.bfloat16))
    pool_input = rounded[:, :pool_width]
    query_matrix = rounded[:, pool_width : pool_width + rec_width].astype(jnp.float32)
    forget_gate_logit = rounded[:, pool_width + rec_width : pool_width + 2 * rec_width].astype(
        jnp.float32
    )
    value_projected = rounded[:, pool_width + 2 * rec_width :].astype(jnp.float32)
    groups_local = pooling_group_maps.shape[0]
    group_size = pooling_group_maps.shape[1]
    reach_rows = 2 ** (groups_local * lax.axis_size("tp"))
    previous = shifted(pool_input[length_total - reach_rows :], "sp", 1)
    extended = jnp.concatenate([previous, pool_input], axis=0).astype(jnp.float32)
    extended = extended.reshape(reach_rows + length_total, groups_local, group_size)
    group_ids = lax.axis_index("tp") * groups_local + jnp.arange(groups_local, dtype=jnp.int32)
    windows = jnp.left_shift(jnp.int32(2), group_ids)
    window_sum = jnp.zeros((length_total, groups_local, group_size), jnp.float32)
    for offset in range(reach_rows):
        inside = (offset < windows).astype(jnp.float32)
        window_sum = (
            window_sum
            + extended[reach_rows - offset : reach_rows - offset + length_total] * inside[:, None]
        )
    position_index = lax.axis_index("sp") * length_total + jnp.arange(length_total, dtype=jnp.int32)
    counts = jnp.minimum(position_index[:, None] + 1, windows[None, :]).astype(jnp.float32)
    pool_diff = (window_sum / counts[:, :, None] - extended[reach_rows:]).astype(jnp.bfloat16)
    pool_mapped = jnp.einsum(
        "tgc,gcd->tgd", pool_diff, pooling_group_maps, preferred_element_type=jnp.float32
    )
    pool_out = (pool_mapped.reshape(length_total, pool_width) * pooling_scale).astype(jnp.bfloat16)
    local_heads = decay_spike.shape[2]
    head_width = rec_width // local_heads
    blocks = length_total // BLOCK
    block_layout = (blocks, BLOCK, local_heads, head_width)
    reader = jax.nn.silu(query_matrix).reshape(block_layout)
    key_gate_value = jax.nn.sigmoid(-lower_bound_logits) * jax.nn.sigmoid(-forget_gate_logit)
    decay_logarithm = (
        jnp.log1p(-key_gate_value).reshape(length_total, local_heads, head_width)
        + decay_spike[0][:, :, None]
    ).reshape(block_layout)
    key_rows = key_gate_value.reshape(block_layout)
    value_rows = value_projected.reshape(block_layout)
    inner_log = jnp.cumsum(decay_logarithm, axis=1)
    read_scaled = reader * jnp.exp(inner_log)
    key_scaled = key_rows * jnp.exp(-inner_log)
    causal = (jnp.arange(BLOCK)[:, None] >= jnp.arange(BLOCK)[None, :]).astype(jnp.float32)
    scores = jnp.einsum("nthd,nshd->nhts", read_scaled, key_scaled, precision=HIGHEST) * causal
    within = jnp.einsum("nhts,nshe->nthe", scores, value_rows, precision=HIGHEST)
    closing = inner_log[:, -1]
    key_tail = key_rows * jnp.exp(closing[:, None] - inner_log)
    deltas = jnp.einsum("nshd,nshe->nhde", key_tail, value_rows, precision=HIGHEST)
    block_decay = jnp.exp(closing)

    def advance(carried, input_batch):
        decay_now, delta_now = input_batch
        return (decay_now[..., None] * carried + delta_now, carried)

    initial = jnp.zeros((local_heads, head_width, head_width), jnp.float32)
    device_state, entry_states = lax.scan(advance, initial, (block_decay, deltas))
    device_decay = jnp.exp(jnp.sum(closing, axis=0))
    scanned = entering(
        (device_decay, device_state),
        "sp",
        join_state,
        (jnp.ones_like(device_decay), jnp.zeros_like(device_state)),
    )
    prior_state = scanned[1]
    before = jnp.cumsum(closing, axis=0) - closing
    start_states = entry_states + jnp.exp(before)[..., None] * prior_state[None]
    read_out = within + jnp.einsum("nthd,nhde->nthe", read_scaled, start_states, precision=HIGHEST)
    read_out = read_out.reshape(length_total, local_heads, head_width)
    recurrent_output = (
        rms_scale(read_out, 1.0).reshape(length_total, rec_width) * head_norm_gain
    ).astype(jnp.bfloat16)
    mixed_rows = jnp.concatenate([pool_out, recurrent_output], axis=1)
    summed = lax.psum_scatter(
        jnp.dot(mixed_rows, out_full, preferred_element_type=jnp.float32).astype(jnp.bfloat16),
        "tp",
        scatter_dimension=0,
        tiled=True,
    )
    return summed[None]


def solution(mesh):
    placed = (
        P("fs", ("sp", "tp"), None),
        P(),
        P("sp", "tp"),
        P("sp", "tp"),
        P("sp", "tp"),
        P("sp", "tp"),
        P("tp", None, None),
        P("tp"),
        P("tp"),
        P("fs", "sp", "tp"),
        P("tp"),
        P("tp", "sp"),
        P("tp", "sp"),
    )
    return jax.shard_map(
        body, mesh=mesh, in_specs=placed, out_specs=P("fs", ("sp", "tp"), None), check_vma=False
    )
```

```python
import jax
import jax.numpy as jnp
from jax import lax
from jax.experimental import pallas as pl
from jax.experimental.pallas import tpu as pltpu
from jax.sharding import PartitionSpec as P

BLOCK = 64


EPSILON = 1e-06
HIGHEST = lax.Precision.HIGHEST


def shifted(value, axis, steps):
    count = lax.axis_size(axis)
    first, last = (max(0, -steps), min(count, count - steps))
    return lax.ppermute(value, axis, [(source, source + steps) for source in range(first, last)])


def entering(shard, axis, join, neutral):
    place = lax.axis_index(axis)
    gathered = jax.tree.map(
        lambda a, kind: lax.all_gather(a.astype(kind), axis), shard, (jnp.bfloat16, jnp.bfloat16)
    )
    state = jax.tree.map(lambda a, e: jnp.zeros_like(a) + jnp.asarray(e, a.dtype), shard, neutral)

    def one(step, state):
        return join(
            state,
            jax.tree.map(
                lambda a, own: lax.dynamic_index_in_dim(a, step, 0, False).astype(own.dtype),
                gathered,
                shard,
            ),
        )

    return lax.fori_loop(0, place, one, state)


def rms_scale(values, gain):
    return values * lax.rsqrt(jnp.mean(values * values, axis=-1, keepdims=True) + EPSILON) * gain


def join_state(earlier, later):
    decay_one, state_one = earlier
    decay_two, state_two = later
    return (decay_one * decay_two, decay_two[..., None] * state_one + state_two)


def swapped(value, axis, bits):
    count = lax.axis_size(axis)
    return lax.ppermute(value, axis, [(source, source ^ bits) for source in range(count)])


def turned(value, axis, steps):
    count = lax.axis_size(axis)
    return lax.ppermute(value, axis, [(source, (source + steps) % count) for source in range(count)])


def picked(stack, place):
    return lax.dynamic_index_in_dim(stack, place, 0, False)


def heads_divide(tokens, query_weight, pooling_input_weight, pooling_group_maps, decay_spike, out_weight):
    planes, members, cores = (lax.axis_size(axis) for axis in ("sp", "fs", "tp"))
    heads = decay_spike.shape[2]
    width = query_weight.shape[1] // heads
    return (
        cores == 2
        and members & (members - 1) == 0
        and heads == planes
        and width % 128 == 0
        and pooling_group_maps.shape[0] * cores == heads
        and pooling_input_weight.shape[1] == query_weight.shape[1]
        and tokens.shape[0] == 1
        and tokens.shape[1] % BLOCK == 0
        and decay_spike.shape[1] == cores * tokens.shape[1] == width
        and query_weight.shape[0] == members * width
        and out_weight.shape[1] == members * width
    )


def pack_kernel(planes, members, width, rows_each, *refs):
    tokens, gain, spikes, maps, scale = refs[:5]
    inputs, outputs = refs[5:9], refs[9:11]
    messages, block, own, rows_out = refs[11 : 11 + planes], *refs[11 + planes : 14 + planes]
    pooling_rows = refs[14 + planes]
    plane, member, core = (lax.axis_index(axis) for axis in ("sp", "fs", "tp"))
    half = width // 2
    heads = spikes.shape[1]
    own_column = lax.rem(2 * plane + core, heads)
    partner_column = lax.rem(2 * plane + 1 - core, heads)
    values = tokens[...].astype(jnp.float32)
    rows_out[pl.ds(0, rows_each), :] = rms_scale(values, gain[...]).astype(jnp.bfloat16)
    rows_out[pl.ds(rows_each, 8), :] = jnp.zeros((8, rows_out.shape[1]), jnp.bfloat16)
    lines = [
        jnp.broadcast_to(spikes[:, n : n + 1], (width, width)).T[:1] for n in range(heads)
    ]
    upper = [line.astype(jnp.bfloat16) for line in lines]
    lower = [
        (line - high.astype(jnp.float32)).astype(jnp.bfloat16) for line, high in zip(lines, upper)
    ]
    rows_out[pl.ds(rows_each, 8), pl.ds(0, width)] = jnp.concatenate(upper + lower, axis=0)
    groups, size = maps.shape[:2]
    for g in range(groups):
        span = pl.ds(g * size, size)
        scaled = maps[g].astype(jnp.float32) * scale[:, span]
        upper = scaled.astype(jnp.bfloat16)
        rest = (scaled - upper.astype(jnp.float32)).astype(jnp.bfloat16)
        rows = outputs[0][span, :]
        pooling_rows[span, :] = (
            jnp.dot(upper, rows, preferred_element_type=jnp.float32)
            + jnp.dot(rest, rows, preferred_element_type=jnp.float32)
        ).astype(jnp.bfloat16)
    outputs = (pooling_rows, outputs[1])
    row = pl.multiple_of(member * width, width)
    for step in range(planes):
        column = pl.multiple_of(lax.rem(plane + step, heads) * width, width)
        for n, w in enumerate(inputs):
            messages[step][pl.ds(0, width), pl.ds(n * width, width)] = w[
                pl.ds(row, width), pl.ds(column, width)
            ]
        for n in range(4):
            top = pl.multiple_of(column + (n % 2) * half, half)
            messages[step][pl.ds(width, half), pl.ds(n * width, width)] = outputs[n // 2][
                pl.ds(top, half), pl.ds(row, width)
            ]
    rows = members * width
    for place, target in ((partner_column, block), (own_column, own)):
        column = pl.multiple_of(place * width, width)
        for n, w in enumerate(inputs):
            target[pl.ds(0, rows), pl.ds(n * width, width)] = w[:, pl.ds(column, width)]
        for n, w in enumerate(outputs):
            target[pl.ds(rows + n * width, width), :] = w[pl.ds(column, width), :]


def down(values, steps):
    rows = lax.broadcasted_iota(jnp.int32, values.shape, 0)
    return jnp.where(rows >= steps, pltpu.roll(values, steps, 0), 0.0)


def layer_kernel(planes, members, cores, width, rows_each, *refs):
    own_vectors, partner_vectors = refs[0], refs[1]
    position = 2
    tokens = [refs[position + n * planes : position + (n + 1) * planes] for n in range(cores)]
    position += cores * planes
    pieces = refs[position : position + members]
    position += members
    blocks = refs[position : position + 2]
    sent, kept = refs[position + 2 : position + 4]
    token_all, weight_in, weight_out, spikes, mixed, sems = refs[position + 4 :]
    plane, member, core = (lax.axis_index(axis) for axis in ("sp", "fs", "tp"))
    column = lax.rem(cores * plane + core, planes)
    owner = lax.div(cores * plane + core, planes)
    owns = owner == core
    length = planes * cores * rows_each
    half = width // 2
    plane_rows = members * width
    copies = []
    for step in range(planes):
        source = lax.rem(plane - step + planes, planes)
        for side in range(cores):
            origin = core if side == 0 else 1 - core
            top = pl.multiple_of((source * cores + origin) * rows_each, rows_each)
            copies.append(
                (
                    tokens[side][step].at[pl.ds(0, rows_each), :],
                    token_all.at[pl.ds(top, rows_each), :],
                )
            )
            copies.append(
                (
                    tokens[side][step].at[pl.ds(rows_each, 8), pl.ds(0, width)],
                    spikes.at[source * cores + origin],
                )
            )
    copy_list = [
        pltpu.make_async_copy(source, target, sems.at[n]) for n, (source, target) in enumerate(copies)
    ]
    for copy in copy_list:
        copy.start()
    used = len(copies)
    own_copies = []
    block_copies = []
    for own_block in blocks:
        block_copies.append(
            [
                pltpu.make_async_copy(
                    own_block.at[pl.ds(0, plane_rows), :],
                    weight_in.at[
                        pl.ds(pl.multiple_of(plane * plane_rows, plane_rows), plane_rows), :
                    ],
                    sems.at[used],
                ),
                pltpu.make_async_copy(
                    own_block.at[pl.ds(plane_rows, 2 * width), :],
                    weight_out.at[
                        :, pl.ds(pl.multiple_of(plane * plane_rows, plane_rows), plane_rows)
                    ],
                    sems.at[used + 1],
                ),
            ]
        )

    @pl.when(owns)
    def _():
        for copy in block_copies[0]:
            copy.start()

    @pl.when(jnp.logical_not(owns))
    def _():
        for copy in block_copies[1]:
            copy.start()

    used += 2
    for bits in range(members):
        for k in range(1, planes):
            source = lax.rem(plane + k, planes)
            place = pl.multiple_of((source * members + (member ^ bits)) * width, width)
            piece = pieces[bits].at[k - 1]
            own_copies.append(
                pltpu.make_async_copy(
                    piece.at[pl.ds(0, width), :], weight_in.at[pl.ds(place, width), :], sems.at[used]
                )
            )
            used += 1
            for n in range(4):
                own_copies.append(
                    pltpu.make_async_copy(
                        piece.at[pl.ds(width, half), pl.ds(n * width, width)],
                        weight_out.at[pl.ds(n * half, half), pl.ds(place, width)],
                        sems.at[used],
                    )
                )
                used += 1
    for copy in own_copies:
        copy.start()
    for copy in copy_list + block_copies[0] + own_copies:
        copy.wait()

    lower_bound, head_gain = (
        jnp.where(owns, own_vectors[pl.ds(n, 1), :], partner_vectors[pl.ds(n, 1), :])
        for n in range(2)
    )
    projected = jnp.dot(token_all[...], weight_in[...], preferred_element_type=jnp.float32)
    projected = projected.astype(jnp.bfloat16).astype(jnp.float32)
    pool_input, query, forget_logit, value = (
        projected[:, n * width : (n + 1) * width] for n in range(4)
    )

    window = jnp.left_shift(jnp.int32(2), plane)
    window_sum = pool_input
    chosen = jnp.zeros_like(pool_input)
    for group in range(planes):
        window_sum = window_sum + down(window_sum, 2**group)
        chosen = jnp.where(plane == group, window_sum, chosen)
    at = lax.broadcasted_iota(jnp.int32, pool_input.shape, 0)
    counts = jnp.minimum(at + 1, window).astype(jnp.float32)
    mixed[:, pl.ds(0, width)] = (chosen / counts - pool_input).astype(jnp.bfloat16)

    spike_row = lax.broadcasted_iota(jnp.int32, (8, width), 0)
    wanted_row = jnp.logical_or(spike_row == column, spike_row == column + planes)
    spike_columns = []
    for source in range(planes):
        parts = spikes[source * cores + owner].astype(jnp.float32)
        line = jnp.sum(jnp.where(wanted_row, parts, 0.0), axis=0, keepdims=True)
        spike_columns.append(jnp.broadcast_to(line, (width, width)).T)
    spike = jnp.concatenate(spike_columns, axis=0)

    reader = query * jax.nn.sigmoid(query)
    key_gate = jax.nn.sigmoid(-lower_bound) * jax.nn.sigmoid(-forget_logit)
    log_decay = jnp.log1p(-key_gate) + spike
    t_at = lax.broadcasted_iota(jnp.int32, (BLOCK, BLOCK), 0)
    s_at = lax.broadcasted_iota(jnp.int32, (BLOCK, BLOCK), 1)
    causal = t_at >= s_at
    lower = causal.astype(jnp.float32)
    state = jnp.zeros((width, width), jnp.float32)
    for n in range(length // BLOCK):
        rows = slice(n * BLOCK, (n + 1) * BLOCK)
        inner_log = jnp.dot(
            lower, log_decay[rows], preferred_element_type=jnp.float32, precision=HIGHEST
        )
        keys = key_gate[rows]
        values = value[rows].astype(jnp.bfloat16)
        read_scaled = (reader[rows] * jnp.exp(inner_log)).astype(jnp.bfloat16)
        key_scaled = (keys * jnp.exp(-inner_log)).astype(jnp.bfloat16)
        scores = lax.dot_general(
            read_scaled, key_scaled, (((1,), (1,)), ((), ())), preferred_element_type=jnp.float32
        )
        scores = jnp.where(causal, scores, 0.0).astype(jnp.bfloat16)
        read = jnp.dot(scores, values, preferred_element_type=jnp.float32)
        read = read + jnp.dot(
            read_scaled, state.astype(jnp.bfloat16), preferred_element_type=jnp.float32
        )
        closing = inner_log[BLOCK - 1 : BLOCK]
        key_tail = (keys * jnp.exp(closing - inner_log)).astype(jnp.bfloat16)
        added = lax.dot_general(
            key_tail, values, (((0,), (0,)), ((), ())), preferred_element_type=jnp.float32
        )
        kept_share = jnp.broadcast_to(jnp.exp(closing), (width, width)).T
        state = kept_share * state + added
        mixed[pl.ds(n * BLOCK, BLOCK), pl.ds(width, width)] = (
            rms_scale(read, 1.0) * head_gain
        ).astype(jnp.bfloat16)
    for p in range(planes):
        for target, side in ((sent, 1 - core), (kept, core)):
            top = pl.multiple_of((p * cores + side) * rows_each, rows_each)
            target[p] = jnp.dot(
                mixed[pl.ds(top, rows_each), :], weight_out[...], preferred_element_type=jnp.float32
            ).astype(jnp.bfloat16)


def by_heads(
    tokens,
    input_norm_gain,
    pooling_input_weight,
    query_weight,
    forget_weight,
    value_weight,
    pooling_group_maps,
    pooling_scale,
    lower_bound_logits,
    decay_spike,
    head_norm_gain,
    pooling_output_weight,
    recurrent_output_weight,
):
    planes, members, cores = (lax.axis_size(axis) for axis in ("sp", "fs", "tp"))
    plane, _, core = (lax.axis_index(axis) for axis in ("sp", "fs", "tp"))
    heads = decay_spike.shape[2]
    head = cores * plane + core
    column = head % heads
    partner_column = (cores * plane + 1 - core) % heads
    width = query_weight.shape[1] // heads
    features = tokens.shape[2]
    rows_each = tokens.shape[1]
    inputs = (pooling_input_weight, query_weight, forget_weight, value_weight)
    outputs = (pooling_output_weight, recurrent_output_weight)
    message = jax.ShapeDtypeStruct((width + width // 2, 4 * width), jnp.bfloat16)
    block = jax.ShapeDtypeStruct(((members + 2) * width, 4 * width), jnp.bfloat16)
    hbm = pl.BlockSpec(memory_space=pl.ANY)
    vmem = pl.BlockSpec(memory_space=pltpu.VMEM)

    def pack(*refs):
        pack_kernel(planes, members, width, rows_each, *refs)

    *messages, partner_block, own_local, own_message = pl.pallas_call(
        pack,
        out_shape=[message] * planes
        + [block] * 2
        + [jax.ShapeDtypeStruct((rows_each + 8, features), jnp.bfloat16)],
        in_specs=[vmem] * 11,
        out_specs=[vmem] * (planes + 3),
        scratch_shapes=[pltpu.VMEM(pooling_output_weight.shape, jnp.bfloat16)],
        name="pack",
    )(
        tokens[0],
        input_norm_gain[None],
        decay_spike[0],
        pooling_group_maps,
        pooling_scale[None],
        *inputs,
        *outputs,
    )

    arrived = []
    for step in range(planes):
        pairs = [
            (p * cores + c, heads * c + (p + step) % heads)
            for p in range(planes)
            for c in range(cores)
        ]
        arrived.append(lax.ppermute(messages[step], ("sp", "tp"), pairs))
    gathered = jnp.stack(arrived)
    others = jnp.stack(
        [picked(gathered, (column - plane - k) % planes) for k in range(1, planes)]
    )
    pieces = [others]
    for bits in range(1, members):
        pieces.append(swapped(others, "fs", bits))
    partner_local = swapped(partner_block, "tp", 1)

    def own_vectors(place):
        return jnp.stack(
            [
                lax.dynamic_slice_in_dim(v, place * width, width, 0)
                for v in (lower_bound_logits, head_norm_gain)
            ]
        )

    received_vectors = swapped(own_vectors(partner_column), "tp", 1)

    own_rows = [own_message]
    for step in range(1, planes):
        own_rows.append(turned(own_message, "sp", step))
    partner_rows = []
    for step in range(planes):
        partner_rows.append(swapped(own_rows[step], "tp", 1))

    length = planes * cores * rows_each

    def layer(*refs):
        layer_kernel(planes, members, cores, width, rows_each, *refs)

    half_shape = jax.ShapeDtypeStruct((planes, rows_each, features), jnp.bfloat16)
    sent, kept = pl.pallas_call(
        layer,
        out_shape=[half_shape, half_shape],
        in_specs=[vmem] * 2 + [hbm] * (cores * planes + members + 2),
        out_specs=[vmem, vmem],
        scratch_shapes=[
            pltpu.VMEM((length, features), jnp.bfloat16),
            pltpu.VMEM((features, 4 * width), jnp.bfloat16),
            pltpu.VMEM((2 * width, planes * members * width), jnp.bfloat16),
            pltpu.VMEM((planes * cores, 8, width), jnp.bfloat16),
            pltpu.VMEM((length, 2 * width), jnp.bfloat16),
            pltpu.SemaphoreType.DMA((2 * cores * planes + 2 + 5 * planes * members,)),
        ],
        name="layer",
    )(
        own_vectors(column),
        received_vectors,
        *own_rows,
        *partner_rows,
        *pieces,
        own_local,
        partner_local,
    )

    from_partner = swapped(sent, "tp", 1)

    def joined(p):
        return picked(kept, p).astype(jnp.float32) + picked(from_partner, p).astype(jnp.float32)

    total = joined(plane)
    for step in range(1, planes):
        portion = joined((plane + step) % planes).astype(jnp.bfloat16)
        total = total + turned(portion, "sp", step).astype(jnp.float32)
    return total.astype(jnp.bfloat16)[None]


def body(*arrays):
    tokens, _, pool_in, query_in, _, _, maps, _, _, spike, _, pool_out, _ = arrays
    if heads_divide(tokens, query_in, pool_in, maps, spike, pool_out):
        return by_heads(*arrays)
    return by_positions(*arrays)


def by_positions(
    tokens,
    input_norm_gain,
    pooling_input_weight,
    query_weight,
    forget_weight,
    value_weight,
    pooling_group_maps,
    pooling_scale,
    lower_bound_logits,
    decay_spike,
    head_norm_gain,
    pooling_output_weight,
    recurrent_output_weight,
):
    gathered = lax.all_gather(tokens, "tp", axis=1, tiled=True)[0]
    length_total = gathered.shape[0]
    normed = rms_scale(gathered.astype(jnp.float32), input_norm_gain).astype(jnp.bfloat16)
    pool_width = pooling_input_weight.shape[1]
    rec_width = query_weight.shape[1]
    stacked = jnp.concatenate(
        [pooling_input_weight, query_weight, forget_weight, value_weight], axis=1
    )
    out_local = jnp.concatenate([pooling_output_weight, recurrent_output_weight], axis=0)
    groups_fs = lax.axis_size("fs")
    member = lax.axis_index("fs")
    slice_width = stacked.shape[1] // groups_fs
    own_slice = lax.dynamic_slice_in_dim(stacked, member * slice_width, slice_width, 1)
    column_part = lax.all_gather(own_slice, "sp", axis=0, tiled=True)
    full_input = lax.all_gather(column_part, "fs", axis=1, tiled=True)
    projected = jnp.dot(normed, full_input, preferred_element_type=jnp.float32)
    slice_height = out_local.shape[0] // groups_fs
    own_rows = lax.dynamic_slice_in_dim(out_local, member * slice_height, slice_height, 0)
    row_part = lax.all_gather(own_rows, "sp", axis=1, tiled=True)
    out_full = lax.all_gather(row_part, "fs", axis=0, tiled=True)
    rounded = lax.optimization_barrier(projected.astype(jnp.bfloat16))
    pool_input = rounded[:, :pool_width]
    query_matrix = rounded[:, pool_width : pool_width + rec_width].astype(jnp.float32)
    forget_gate_logit = rounded[:, pool_width + rec_width : pool_width + 2 * rec_width].astype(
        jnp.float32
    )
    value_projected = rounded[:, pool_width + 2 * rec_width :].astype(jnp.float32)
    groups_local = pooling_group_maps.shape[0]
    group_size = pooling_group_maps.shape[1]
    reach_rows = 2 ** (groups_local * lax.axis_size("tp"))
    previous = shifted(pool_input[length_total - reach_rows :], "sp", 1)
    extended = jnp.concatenate([previous, pool_input], axis=0).astype(jnp.float32)
    extended = extended.reshape(reach_rows + length_total, groups_local, group_size)
    group_ids = lax.axis_index("tp") * groups_local + jnp.arange(groups_local, dtype=jnp.int32)
    windows = jnp.left_shift(jnp.int32(2), group_ids)
    window_sum = jnp.zeros((length_total, groups_local, group_size), jnp.float32)
    for offset in range(reach_rows):
        inside = (offset < windows).astype(jnp.float32)
        window_sum = (
            window_sum
            + extended[reach_rows - offset : reach_rows - offset + length_total] * inside[:, None]
        )
    position_index = lax.axis_index("sp") * length_total + jnp.arange(length_total, dtype=jnp.int32)
    counts = jnp.minimum(position_index[:, None] + 1, windows[None, :]).astype(jnp.float32)
    pool_diff = (window_sum / counts[:, :, None] - extended[reach_rows:]).astype(jnp.bfloat16)
    pool_mapped = jnp.einsum(
        "tgc,gcd->tgd", pool_diff, pooling_group_maps, preferred_element_type=jnp.float32
    )
    pool_out = (pool_mapped.reshape(length_total, pool_width) * pooling_scale).astype(jnp.bfloat16)
    local_heads = decay_spike.shape[2]
    head_width = rec_width // local_heads
    blocks = length_total // BLOCK
    block_layout = (blocks, BLOCK, local_heads, head_width)
    reader = jax.nn.silu(query_matrix).reshape(block_layout)
    key_gate_value = jax.nn.sigmoid(-lower_bound_logits) * jax.nn.sigmoid(-forget_gate_logit)
    decay_logarithm = (
        jnp.log1p(-key_gate_value).reshape(length_total, local_heads, head_width)
        + decay_spike[0][:, :, None]
    ).reshape(block_layout)
    key_rows = key_gate_value.reshape(block_layout)
    value_rows = value_projected.reshape(block_layout)
    inner_log = jnp.cumsum(decay_logarithm, axis=1)
    read_scaled = reader * jnp.exp(inner_log)
    key_scaled = key_rows * jnp.exp(-inner_log)
    causal = (jnp.arange(BLOCK)[:, None] >= jnp.arange(BLOCK)[None, :]).astype(jnp.float32)
    scores = jnp.einsum("nthd,nshd->nhts", read_scaled, key_scaled, precision=HIGHEST) * causal
    within = jnp.einsum("nhts,nshe->nthe", scores, value_rows, precision=HIGHEST)
    closing = inner_log[:, -1]
    key_tail = key_rows * jnp.exp(closing[:, None] - inner_log)
    deltas = jnp.einsum("nshd,nshe->nhde", key_tail, value_rows, precision=HIGHEST)
    block_decay = jnp.exp(closing)

    def advance(carried, input_batch):
        decay_now, delta_now = input_batch
        return (decay_now[..., None] * carried + delta_now, carried)

    initial = jnp.zeros((local_heads, head_width, head_width), jnp.float32)
    device_state, entry_states = lax.scan(advance, initial, (block_decay, deltas))
    device_decay = jnp.exp(jnp.sum(closing, axis=0))
    scanned = entering(
        (device_decay, device_state),
        "sp",
        join_state,
        (jnp.ones_like(device_decay), jnp.zeros_like(device_state)),
    )
    prior_state = scanned[1]
    before = jnp.cumsum(closing, axis=0) - closing
    start_states = entry_states + jnp.exp(before)[..., None] * prior_state[None]
    read_out = within + jnp.einsum("nthd,nhde->nthe", read_scaled, start_states, precision=HIGHEST)
    read_out = read_out.reshape(length_total, local_heads, head_width)
    recurrent_output = (
        rms_scale(read_out, 1.0).reshape(length_total, rec_width) * head_norm_gain
    ).astype(jnp.bfloat16)
    mixed_rows = jnp.concatenate([pool_out, recurrent_output], axis=1)
    summed = lax.psum_scatter(
        jnp.dot(mixed_rows, out_full, preferred_element_type=jnp.float32).astype(jnp.bfloat16),
        "tp",
        scatter_dimension=0,
        tiled=True,
    )
    return summed[None]


def solution(mesh):
    placed = (
        P("fs", ("sp", "tp"), None),
        P(),
        P("sp", "tp"),
        P("sp", "tp"),
        P("sp", "tp"),
        P("sp", "tp"),
        P("tp", None, None),
        P("tp"),
        P("tp"),
        P("fs", "sp", "tp"),
        P("tp"),
        P("tp", "sp"),
        P("tp", "sp"),
    )
    return jax.shard_map(
        body, mesh=mesh, in_specs=placed, out_specs=P("fs", ("sp", "tp"), None), check_vma=False
    )
```

```python
import jax
import jax.numpy as jnp
from jax import lax
from jax.experimental import pallas as pl
from jax.experimental.pallas import tpu as pltpu
from jax.sharding import PartitionSpec as P

BLOCK = 64


EPSILON = 1e-06
HIGHEST = lax.Precision.HIGHEST


def shifted(value, axis, steps):
    count = lax.axis_size(axis)
    first, last = (max(0, -steps), min(count, count - steps))
    return lax.ppermute(value, axis, [(source, source + steps) for source in range(first, last)])


def entering(shard, axis, join, neutral):
    place = lax.axis_index(axis)
    gathered = jax.tree.map(
        lambda a, kind: lax.all_gather(a.astype(kind), axis), shard, (jnp.bfloat16, jnp.bfloat16)
    )
    state = jax.tree.map(lambda a, e: jnp.zeros_like(a) + jnp.asarray(e, a.dtype), shard, neutral)

    def one(step, state):
        return join(
            state,
            jax.tree.map(
                lambda a, own: lax.dynamic_index_in_dim(a, step, 0, False).astype(own.dtype),
                gathered,
                shard,
            ),
        )

    return lax.fori_loop(0, place, one, state)


def rms_scale(values, gain):
    return values * lax.rsqrt(jnp.mean(values * values, axis=-1, keepdims=True) + EPSILON) * gain


def join_state(earlier, later):
    decay_one, state_one = earlier
    decay_two, state_two = later
    return (decay_one * decay_two, decay_two[..., None] * state_one + state_two)


def swapped(value, axis, bits):
    count = lax.axis_size(axis)
    return lax.ppermute(value, axis, [(source, source ^ bits) for source in range(count)])


def picked(stack, place, axis=0):
    return lax.dynamic_index_in_dim(stack, place, axis, False)


def halves_divide(tokens, query_weight, pooling_input_weight, pooling_group_maps, decay_spike, out_weight):
    planes, members, cores = (lax.axis_size(axis) for axis in ("sp", "fs", "tp"))
    heads = decay_spike.shape[2]
    width = query_weight.shape[1] // heads
    return (
        cores == 2
        and planes == 2 * cores
        and members == 2 * cores
        and heads == 2 * cores
        and width % 128 == 0
        and pooling_group_maps.shape[0] * 2 == heads
        and pooling_input_weight.shape[1] == query_weight.shape[1]
        and tokens.shape[0] == 1
        and tokens.shape[1] % BLOCK == 0
        and decay_spike.shape[1] == cores * tokens.shape[1] == width
        and query_weight.shape[0] == heads * width
        and out_weight.shape[1] == heads * width
        and 2 ** (2 * pooling_group_maps.shape[0]) <= HALO
    )


HALO = 16


def places():
    plane, member, core = (lax.axis_index(axis) for axis in ("sp", "fs", "tp"))
    late, half = lax.div(plane, 2), lax.rem(plane, 2)
    row, side = lax.div(member, 2), lax.rem(member, 2)
    return plane, late, half, row, side, core


def first_kernel(width, rows_each, *refs):
    tokens, gain, spikes = refs[:3]
    inputs, messages, rows_out, sems = refs[3:7], refs[7:9], refs[9], refs[10]
    _, _, half, row, side, core = places()
    part = inputs[0].shape[0] // 2
    top = pl.multiple_of(side * part, part)
    first = jnp.where(core == half, 0, 1)
    copies = []
    for n in range(2):
        place = 2 * row + jnp.where(n == 0, first, 1 - first)
        column = pl.multiple_of(place * width, width)
        for m, w in enumerate(inputs):
            copies.append(
                pltpu.make_async_copy(
                    w.at[pl.ds(top, part), pl.ds(column, width)],
                    messages[n].at[:, pl.ds(m * width, width)],
                    sems.at[n * 4 + m],
                )
            )
    for copy in copies:
        copy.start()
    values = tokens[...].astype(jnp.float32)
    rows_out[pl.ds(0, rows_each), :] = rms_scale(values, gain[...]).astype(jnp.bfloat16)
    rows_out[pl.ds(rows_each, 8), :] = jnp.zeros((8, rows_out.shape[1]), jnp.bfloat16)
    upper = spikes[...].astype(jnp.bfloat16)
    lower = (spikes[...] - upper.astype(jnp.float32)).astype(jnp.bfloat16)
    rows_out[pl.ds(rows_each, 8), pl.ds(0, width)] = jnp.concatenate([upper, lower], axis=0)
    for copy in copies:
        copy.wait()


def pack_kernel(width, *refs):
    maps, scale, bound, head_gain = refs[:4]
    inputs, outputs = refs[4:8], refs[8:10]
    out_messages, block, own, own_vectors, partner_vectors, pooling_rows, sems = (
        refs[10:12],
        *refs[12:],
    )
    _, _, half, row, side, core = places()
    part = inputs[0].shape[0] // 2
    rows = 2 * part
    ends = ((2 * row + 1 - core, block), (2 * row + core, own))
    copies = []
    for n, (place, target) in enumerate(ends):
        column = pl.multiple_of(place * width, width)
        for m, w in enumerate(inputs):
            copies.append(
                pltpu.make_async_copy(
                    w.at[:, pl.ds(column, width)],
                    target.at[pl.ds(0, rows), pl.ds(m * width, width)],
                    sems.at[n * 4 + m],
                )
            )
    for copy in copies:
        copy.start()
    for place, target in ((2 * row + core, own_vectors), (2 * row + 1 - core, partner_vectors)):
        column = pl.ds(pl.multiple_of(place * width, width), width)
        for n, vector in enumerate((bound, head_gain)):
            target[pl.ds(n, 1), :] = vector[:, column]
    groups, size = maps.shape[:2]
    for g in range(groups):
        span = pl.ds(g * size, size)
        scaled = maps[g].astype(jnp.float32) * scale[:, span]
        high = scaled.astype(jnp.bfloat16)
        rest = (scaled - high.astype(jnp.float32)).astype(jnp.bfloat16)
        pooled = outputs[0][span, :]
        pooling_rows[span, :] = (
            jnp.dot(high, pooled, preferred_element_type=jnp.float32)
            + jnp.dot(rest, pooled, preferred_element_type=jnp.float32)
        ).astype(jnp.bfloat16)
    outputs = (pooling_rows, outputs[1])
    top = pl.multiple_of(side * part, part)
    first = jnp.where(core == half, 0, 1)
    for n in range(2):
        place = 2 * row + jnp.where(n == 0, first, 1 - first)
        column = pl.multiple_of(place * width, width)
        for m, w in enumerate(outputs):
            out_messages[n][pl.ds(m * width, width), :] = w[pl.ds(column, width), pl.ds(top, part)]
    for place, target in ends:
        column = pl.multiple_of(place * width, width)
        for m, w in enumerate(outputs):
            target[pl.ds(rows + m * width, width), :] = w[pl.ds(column, width), :]
    for copy in copies:
        copy.wait()


def down(values, steps):
    rows = lax.broadcasted_iota(jnp.int32, values.shape, 0)
    return jnp.where(rows >= steps, pltpu.roll(values, steps, 0), 0.0)


def piece_sources(pieces, plane, core):
    planes = lax.axis_size("sp")
    near, far, third = pieces[0:2], pieces[2:4], (pieces[4:6], pieces[6:8])
    always = [(near, lax.rem(plane + 2 - core, planes)), (far, lax.rem(plane + 1 + core, planes))]
    last = lax.rem(plane + 3, planes)
    return always, third, last


def start_pieces(pieces, blocks, sems, used, plane, side, core, owns, piece_target, block_target):
    always, third, last = piece_sources(pieces, plane, core)
    waits = []

    def copies(pair, source, slot):
        return [
            pltpu.make_async_copy(
                pair[n], piece_target(source, side if n == 0 else 1 - side), sems.at[slot + n]
            )
            for n in range(2)
        ]

    for pair, source in always:
        group = copies(pair, source, used)
        for copy in group:
            copy.start()
        waits += group
        used += 2
    choices = [copies(pair, last, used) for pair in third]
    for n in range(2):

        @pl.when(core == n)
        def _(n=n):
            for copy in choices[n]:
                copy.start()

    waits += choices[0]
    used += 2
    own = [pltpu.make_async_copy(block_target(b)[0], block_target(b)[1], sems.at[used]) for b in blocks]
    for n in range(2):

        @pl.when(owns if n == 0 else jnp.logical_not(owns))
        def _(n=n):
            own[n].start()

    waits.append(own[0])
    return waits, used + 1


def state_kernel(width, rows_each, *refs):
    own_vectors, partner_vectors = refs[:2]
    tokens, pieces, blocks = refs[2:10], refs[10:18], refs[18:20]
    read_local, read_full, pool_rows, carry = refs[20:24]
    token_all, weight_in, spikes, sems = refs[24:]
    plane, _, half, row, side, core = places()
    owns = core == half
    column = 2 * row + core
    plane_rows = 4 * width
    part = plane_rows // 2
    waits = []
    used = 0
    for a in range(2):
        for b in range(2):
            for c in range(2):
                piece = tokens[(a * 2 + b) * 2 + c]
                order = ((row ^ b) * 2 + (half ^ a)) * 2 + (core ^ c)
                top = pl.multiple_of(order * rows_each, rows_each)
                waits.append(
                    pltpu.make_async_copy(
                        piece.at[pl.ds(0, rows_each), :],
                        token_all.at[pl.ds(top, rows_each), :],
                        sems.at[used],
                    )
                )
                waits.append(
                    pltpu.make_async_copy(
                        piece.at[pl.ds(rows_each, 8), pl.ds(0, width)],
                        spikes.at[order],
                        sems.at[used + 1],
                    )
                )
                used += 2
    for copy in waits:
        copy.start()

    def piece_target(source, x):
        return weight_in.at[pl.ds(pl.multiple_of(source * plane_rows + x * part, part), part), :]

    def block_target(block):
        return (
            block.at[pl.ds(0, plane_rows), :],
            weight_in.at[pl.ds(pl.multiple_of(plane * plane_rows, plane_rows), plane_rows), :],
        )

    more, used = start_pieces(
        pieces, blocks, sems, used, plane, side, core, owns, piece_target, block_target
    )
    for copy in waits + more:
        copy.wait()
    lower_bound = jnp.where(owns, own_vectors[pl.ds(0, 1), :], partner_vectors[pl.ds(0, 1), :])
    projected = jnp.dot(token_all[...], weight_in[...], preferred_element_type=jnp.float32)
    projected = projected.astype(jnp.bfloat16)
    pool_rows[...] = projected[:, :width]
    query, forget_logit, value = (
        projected[:, n * width : (n + 1) * width].astype(jnp.float32) for n in range(1, 4)
    )
    spike_row = lax.broadcasted_iota(jnp.int32, (8, width), 0)
    wanted_row = jnp.logical_or(spike_row == column, spike_row == column + 4)
    spike_columns = []
    for n in range(4):
        parts = spikes[2 * n + half].astype(jnp.float32)
        line = jnp.sum(jnp.where(wanted_row, parts, 0.0), axis=0, keepdims=True)
        spike_columns.append(jnp.broadcast_to(line, (width, width)).T)
    spike = jnp.concatenate(spike_columns, axis=0)
    reader = query * jax.nn.sigmoid(query)
    key_gate = jax.nn.sigmoid(-lower_bound) * jax.nn.sigmoid(-forget_logit)
    log_decay = jnp.log1p(-key_gate) + spike
    t_at = lax.broadcasted_iota(jnp.int32, (BLOCK, BLOCK), 0)
    s_at = lax.broadcasted_iota(jnp.int32, (BLOCK, BLOCK), 1)
    causal = t_at >= s_at
    lower = causal.astype(jnp.float32)
    length = 4 * rows_each
    states = [jnp.zeros((width, width), jnp.float32)] * 2
    before = [jnp.zeros((1, width), jnp.float32)] * 2
    for n in range(length // BLOCK):
        for seq in range(2):
            begin = seq * length + n * BLOCK
            rows = slice(begin, begin + BLOCK)
            inner_log = jnp.dot(
                lower, log_decay[rows], preferred_element_type=jnp.float32, precision=HIGHEST
            )
            keys = key_gate[rows]
            values = value[rows].astype(jnp.bfloat16)
            grown = reader[rows] * jnp.exp(inner_log)
            read_scaled = grown.astype(jnp.bfloat16)
            key_scaled = (keys * jnp.exp(-inner_log)).astype(jnp.bfloat16)
            scores = lax.dot_general(
                read_scaled, key_scaled, (((1,), (1,)), ((), ())), preferred_element_type=jnp.float32
            )
            scores = jnp.where(causal, scores, 0.0).astype(jnp.bfloat16)
            read = jnp.dot(scores, values, preferred_element_type=jnp.float32)
            if n > 0:
                read = read + jnp.dot(
                    read_scaled,
                    states[seq].astype(jnp.bfloat16),
                    preferred_element_type=jnp.float32,
                )
            closing = inner_log[BLOCK - 1 : BLOCK]
            key_tail = (keys * jnp.exp(closing - inner_log)).astype(jnp.bfloat16)
            added = lax.dot_general(
                key_tail, values, (((0,), (0,)), ((), ())), preferred_element_type=jnp.float32
            )
            share = jnp.broadcast_to(jnp.exp(closing), (width, width)).T
            states[seq] = share * states[seq] + added
            read_local[pl.ds(begin, BLOCK), :] = read
            read_full[pl.ds(begin, BLOCK), :] = (grown * jnp.exp(before[seq])).astype(jnp.bfloat16)
            before[seq] = before[seq] + closing
    for seq in range(2):
        top = seq * (width + HALO)
        carry[pl.ds(top, width), :] = states[seq].astype(jnp.bfloat16)
        carry[pl.ds(top + width, HALO), :] = projected[
            (seq + 1) * length - HALO : (seq + 1) * length, :width
        ]


def output_kernel(width, rows_each, *refs):
    own_vectors, partner_vectors, read_local, read_full, pool_rows, carry = refs[:6]
    pieces, blocks = refs[6:14], refs[14:16]
    sent, kept = refs[16:18]
    weight_out, mixed, sems = refs[18:]
    plane, late, half, row, side, core = places()
    owns = core == half
    plane_rows = 4 * width
    part = plane_rows // 2
    length = 4 * rows_each

    def piece_target(source, x):
        return weight_out.at[:, pl.ds(pl.multiple_of(source * plane_rows + x * part, part), part)]

    def block_target(block):
        return (
            block.at[pl.ds(plane_rows, 2 * width), :],
            weight_out.at[:, pl.ds(pl.multiple_of(plane * plane_rows, plane_rows), plane_rows)],
        )

    waits, _ = start_pieces(
        pieces, blocks, sems, 0, plane, side, core, owns, piece_target, block_target
    )
    head_gain = jnp.where(owns, own_vectors[pl.ds(1, 1), :], partner_vectors[pl.ds(1, 1), :])
    group = 2 * half + row
    window = jnp.left_shift(jnp.int32(2), group)
    for seq in range(2):
        top = seq * (width + HALO)
        rows = pl.ds(seq * length, length)
        extended = jnp.concatenate(
            [carry[pl.ds(top + width, HALO), :], pool_rows[rows, :]], axis=0
        ).astype(jnp.float32)
        window_sum = extended
        chosen = jnp.zeros_like(extended)
        for g in range(4):
            window_sum = window_sum + down(window_sum, 2**g)
            chosen = jnp.where(group == g, window_sum, chosen)
        at = lax.broadcasted_iota(jnp.int32, (length, width), 0) + late * length
        counts = jnp.minimum(at + 1, window).astype(jnp.float32)
        mixed[rows, pl.ds(0, width)] = (chosen[HALO:] / counts - extended[HALO:]).astype(
            jnp.bfloat16
        )
        read = read_local[rows, :] + jnp.dot(
            read_full[rows, :], carry[pl.ds(top, width), :], preferred_element_type=jnp.float32
        )
        mixed[rows, pl.ds(width, width)] = (rms_scale(read, 1.0) * head_gain).astype(jnp.bfloat16)
    for copy in waits:
        copy.wait()
    for target, c in ((sent, 1 - core), (kept, core)):
        for n in range(4):
            top = pl.multiple_of((n * 2 + c) * rows_each, rows_each)
            target[n // 2, n % 2] = jnp.dot(
                mixed[pl.ds(top, rows_each), :], weight_out[...], preferred_element_type=jnp.float32
            ).astype(jnp.bfloat16)


def by_halves(
    tokens,
    input_norm_gain,
    pooling_input_weight,
    query_weight,
    forget_weight,
    value_weight,
    pooling_group_maps,
    pooling_scale,
    lower_bound_logits,
    decay_spike,
    head_norm_gain,
    pooling_output_weight,
    recurrent_output_weight,
):
    planes, members, cores = (lax.axis_size(axis) for axis in ("sp", "fs", "tp"))
    _, _, half, row, _, _ = places()
    heads = decay_spike.shape[2]
    width = query_weight.shape[1] // heads
    features = tokens.shape[2]
    rows_each = tokens.shape[1]
    part = query_weight.shape[0] // 2
    hbm = pl.BlockSpec(memory_space=pl.ANY)
    vmem = pl.BlockSpec(memory_space=pltpu.VMEM)

    def made(*shape, kind=jnp.bfloat16):
        return jax.ShapeDtypeStruct(shape, kind)

    def pack(*refs):
        pack_kernel(width, *refs)

    weights_in = (pooling_input_weight, query_weight, forget_weight, value_weight)

    def first(*refs):
        first_kernel(width, rows_each, *refs)

    *messages, own_rows = pl.pallas_call(
        first,
        out_shape=[made(part, 4 * width)] * 2 + [made(rows_each + 8, features)],
        in_specs=[vmem] * 3 + [hbm] * 4,
        out_specs=[vmem] * 3,
        scratch_shapes=[pltpu.SemaphoreType.DMA((8,))],
        name="first",
    )(tokens[0], input_norm_gain[None], decay_spike[0].T, *weights_in)
    block = made(2 * part + 2 * width, 4 * width)
    *out_messages, partner_block, own_local, vectors, partner_vectors = pl.pallas_call(
        pack,
        out_shape=[made(2 * width, part)] * 2
        + [block] * 2
        + [made(2, width, kind=jnp.float32)] * 2,
        in_specs=[vmem] * 4 + [hbm] * 4 + [vmem] * 2,
        out_specs=[vmem] * 6,
        scratch_shapes=[
            pltpu.VMEM(pooling_output_weight.shape, jnp.bfloat16),
            pltpu.SemaphoreType.DMA((8,)),
        ],
        name="pack",
    )(
        pooling_group_maps,
        pooling_scale[None],
        lower_bound_logits[None],
        head_norm_gain[None],
        *weights_in,
        pooling_output_weight,
        recurrent_output_weight,
    )

    def hops(wanted):
        return [
            (((p + k) % planes) * cores + p % cores, p * cores + c)
            for p in range(planes)
            for k, c in wanted
        ]

    rounds = (
        (0, hops([(2, 0), (1, 1)])),
        (1, hops([(2, 1), (1, 0)])),
        (1, hops([(3, 0)])),
        (0, hops([(3, 1)])),
    )

    def shared(pair):
        pieces = []
        for n, (which, pairs) in enumerate(rounds):
            arrived = lax.ppermute(pair[which], ("sp", "tp"), pairs)
            pieces.append(arrived)
            used = range(cores) if n < 2 else (n - 2,)
            across = [(f * cores + c, (f ^ 1) * cores + c) for f in range(members) for c in used]
            pieces.append(lax.ppermute(arrived, ("fs", "tp"), across))
        return pieces

    input_pieces = shared(messages)
    output_pieces = shared(out_messages)
    partner_local = swapped(partner_block, "tp", 1)

    received_vectors = swapped(partner_vectors, "tp", 1)
    other_rows = swapped(own_rows, "sp", 1)
    chip_rows = []
    for rows in (own_rows, other_rows):
        chip_rows += [rows, swapped(rows, "fs", 2)]
    token_pieces = []
    for rows in chip_rows:
        token_pieces += [rows, swapped(rows, "tp", 1)]

    length = 8 * rows_each
    carry_shape = made(2 * (width + HALO), width)

    def state(*refs):
        state_kernel(width, rows_each, *refs)

    read_local, read_full, pool_rows, carry = pl.pallas_call(
        state,
        out_shape=[
            made(length, width, kind=jnp.float32),
            made(length, width),
            made(length, width),
            carry_shape,
        ],
        in_specs=[vmem] * 2 + [hbm] * 18,
        out_specs=[vmem] * 4,
        scratch_shapes=[
            pltpu.VMEM((length, features), jnp.bfloat16),
            pltpu.VMEM((features, 4 * width), jnp.bfloat16),
            pltpu.VMEM((8, 8, width), jnp.bfloat16),
            pltpu.SemaphoreType.DMA((23,)),
        ],
        name="state",
    )(vectors, received_vectors, *token_pieces, *input_pieces, own_local, partner_local)
    entering_carry = lax.ppermute(carry, "sp", [(p, p + 2) for p in range(planes - 2)])

    def output(*refs):
        output_kernel(width, rows_each, *refs)

    half_shape = made(2, 2, rows_each, features)
    sent, kept = pl.pallas_call(
        output,
        out_shape=[half_shape] * 2,
        in_specs=[vmem] * 6 + [hbm] * 10,
        out_specs=[vmem] * 2,
        scratch_shapes=[
            pltpu.VMEM((2 * width, features), jnp.bfloat16),
            pltpu.VMEM((length, 2 * width), jnp.bfloat16),
            pltpu.SemaphoreType.DMA((7,)),
        ],
        name="output",
    )(
        vectors,
        received_vectors,
        read_local,
        read_full,
        pool_rows,
        entering_carry,
        *output_pieces,
        own_local,
        partner_local,
    )
    from_partner = swapped(sent, "tp", 1)
    middle = features // 2

    def joined(place, axis, columns):
        return sum(
            picked(v[..., columns], place, axis).astype(jnp.float32) for v in (kept, from_partner)
        )

    left, right = slice(0, middle), slice(middle, features)
    left_in = swapped(joined(1 - row, 0, left).astype(jnp.bfloat16), "fs", 2)
    right_in = swapped(joined(1 - half, 1, right).astype(jnp.bfloat16), "sp", 1)
    left_sum = joined(row, 0, left) + left_in.astype(jnp.float32)
    right_sum = joined(half, 1, right) + right_in.astype(jnp.float32)
    left_last = swapped(picked(left_sum, 1 - half).astype(jnp.bfloat16), "sp", 1)
    right_last = swapped(picked(right_sum, 1 - row).astype(jnp.bfloat16), "fs", 2)
    left_total = picked(left_sum, half) + left_last.astype(jnp.float32)
    right_total = picked(right_sum, row) + right_last.astype(jnp.float32)
    total = jnp.concatenate([left_total, right_total], axis=1)
    return total.astype(jnp.bfloat16)[None]


def body(*arrays):
    tokens, _, pool_in, query_in, _, _, maps, _, _, spike, _, pool_out, _ = arrays
    if halves_divide(tokens, query_in, pool_in, maps, spike, pool_out):
        return by_halves(*arrays)
    return by_positions(*arrays)


def by_positions(
    tokens,
    input_norm_gain,
    pooling_input_weight,
    query_weight,
    forget_weight,
    value_weight,
    pooling_group_maps,
    pooling_scale,
    lower_bound_logits,
    decay_spike,
    head_norm_gain,
    pooling_output_weight,
    recurrent_output_weight,
):
    gathered = lax.all_gather(tokens, "tp", axis=1, tiled=True)[0]
    length_total = gathered.shape[0]
    normed = rms_scale(gathered.astype(jnp.float32), input_norm_gain).astype(jnp.bfloat16)
    pool_width = pooling_input_weight.shape[1]
    rec_width = query_weight.shape[1]
    stacked = jnp.concatenate(
        [pooling_input_weight, query_weight, forget_weight, value_weight], axis=1
    )
    out_local = jnp.concatenate([pooling_output_weight, recurrent_output_weight], axis=0)
    groups_fs = lax.axis_size("fs")
    member = lax.axis_index("fs")
    slice_width = stacked.shape[1] // groups_fs
    own_slice = lax.dynamic_slice_in_dim(stacked, member * slice_width, slice_width, 1)
    column_part = lax.all_gather(own_slice, "sp", axis=0, tiled=True)
    full_input = lax.all_gather(column_part, "fs", axis=1, tiled=True)
    projected = jnp.dot(normed, full_input, preferred_element_type=jnp.float32)
    slice_height = out_local.shape[0] // groups_fs
    own_rows = lax.dynamic_slice_in_dim(out_local, member * slice_height, slice_height, 0)
    row_part = lax.all_gather(own_rows, "sp", axis=1, tiled=True)
    out_full = lax.all_gather(row_part, "fs", axis=0, tiled=True)
    rounded = lax.optimization_barrier(projected.astype(jnp.bfloat16))
    pool_input = rounded[:, :pool_width]
    query_matrix = rounded[:, pool_width : pool_width + rec_width].astype(jnp.float32)
    forget_gate_logit = rounded[:, pool_width + rec_width : pool_width + 2 * rec_width].astype(
        jnp.float32
    )
    value_projected = rounded[:, pool_width + 2 * rec_width :].astype(jnp.float32)
    groups_local = pooling_group_maps.shape[0]
    group_size = pooling_group_maps.shape[1]
    reach_rows = 2 ** (groups_local * lax.axis_size("tp"))
    previous = shifted(pool_input[length_total - reach_rows :], "sp", 1)
    extended = jnp.concatenate([previous, pool_input], axis=0).astype(jnp.float32)
    extended = extended.reshape(reach_rows + length_total, groups_local, group_size)
    group_ids = lax.axis_index("tp") * groups_local + jnp.arange(groups_local, dtype=jnp.int32)
    windows = jnp.left_shift(jnp.int32(2), group_ids)
    window_sum = jnp.zeros((length_total, groups_local, group_size), jnp.float32)
    for offset in range(reach_rows):
        inside = (offset < windows).astype(jnp.float32)
        window_sum = (
            window_sum
            + extended[reach_rows - offset : reach_rows - offset + length_total] * inside[:, None]
        )
    position_index = lax.axis_index("sp") * length_total + jnp.arange(length_total, dtype=jnp.int32)
    counts = jnp.minimum(position_index[:, None] + 1, windows[None, :]).astype(jnp.float32)
    pool_diff = (window_sum / counts[:, :, None] - extended[reach_rows:]).astype(jnp.bfloat16)
    pool_mapped = jnp.einsum(
        "tgc,gcd->tgd", pool_diff, pooling_group_maps, preferred_element_type=jnp.float32
    )
    pool_out = (pool_mapped.reshape(length_total, pool_width) * pooling_scale).astype(jnp.bfloat16)
    local_heads = decay_spike.shape[2]
    head_width = rec_width // local_heads
    blocks = length_total // BLOCK
    block_layout = (blocks, BLOCK, local_heads, head_width)
    reader = jax.nn.silu(query_matrix).reshape(block_layout)
    key_gate_value = jax.nn.sigmoid(-lower_bound_logits) * jax.nn.sigmoid(-forget_gate_logit)
    decay_logarithm = (
        jnp.log1p(-key_gate_value).reshape(length_total, local_heads, head_width)
        + decay_spike[0][:, :, None]
    ).reshape(block_layout)
    key_rows = key_gate_value.reshape(block_layout)
    value_rows = value_projected.reshape(block_layout)
    inner_log = jnp.cumsum(decay_logarithm, axis=1)
    read_scaled = reader * jnp.exp(inner_log)
    key_scaled = key_rows * jnp.exp(-inner_log)
    causal = (jnp.arange(BLOCK)[:, None] >= jnp.arange(BLOCK)[None, :]).astype(jnp.float32)
    scores = jnp.einsum("nthd,nshd->nhts", read_scaled, key_scaled, precision=HIGHEST) * causal
    within = jnp.einsum("nhts,nshe->nthe", scores, value_rows, precision=HIGHEST)
    closing = inner_log[:, -1]
    key_tail = key_rows * jnp.exp(closing[:, None] - inner_log)
    deltas = jnp.einsum("nshd,nshe->nhde", key_tail, value_rows, precision=HIGHEST)
    block_decay = jnp.exp(closing)

    def advance(carried, input_batch):
        decay_now, delta_now = input_batch
        return (decay_now[..., None] * carried + delta_now, carried)

    initial = jnp.zeros((local_heads, head_width, head_width), jnp.float32)
    device_state, entry_states = lax.scan(advance, initial, (block_decay, deltas))
    device_decay = jnp.exp(jnp.sum(closing, axis=0))
    scanned = entering(
        (device_decay, device_state),
        "sp",
        join_state,
        (jnp.ones_like(device_decay), jnp.zeros_like(device_state)),
    )
    prior_state = scanned[1]
    before = jnp.cumsum(closing, axis=0) - closing
    start_states = entry_states + jnp.exp(before)[..., None] * prior_state[None]
    read_out = within + jnp.einsum("nthd,nhde->nthe", read_scaled, start_states, precision=HIGHEST)
    read_out = read_out.reshape(length_total, local_heads, head_width)
    recurrent_output = (
        rms_scale(read_out, 1.0).reshape(length_total, rec_width) * head_norm_gain
    ).astype(jnp.bfloat16)
    mixed_rows = jnp.concatenate([pool_out, recurrent_output], axis=1)
    summed = lax.psum_scatter(
        jnp.dot(mixed_rows, out_full, preferred_element_type=jnp.float32).astype(jnp.bfloat16),
        "tp",
        scatter_dimension=0,
        tiled=True,
    )
    return summed[None]


def solution(mesh):
    placed = (
        P("fs", ("sp", "tp"), None),
        P(),
        P("sp", "tp"),
        P("sp", "tp"),
        P("sp", "tp"),
        P("sp", "tp"),
        P("tp", None, None),
        P("tp"),
        P("tp"),
        P("fs", "sp", "tp"),
        P("tp"),
        P("tp", "sp"),
        P("tp", "sp"),
    )
    return jax.shard_map(
        body, mesh=mesh, in_specs=placed, out_specs=P("fs", ("sp", "tp"), None), check_vma=False
    )
```

```python
import jax
import jax.numpy as jnp
from jax import lax
from jax.experimental import pallas as pl
from jax.experimental.pallas import tpu as pltpu
from jax.sharding import PartitionSpec as P

BLOCK = 64


EPSILON = 1e-06
HIGHEST = lax.Precision.HIGHEST


def shifted(value, axis, steps):
    count = lax.axis_size(axis)
    first, last = (max(0, -steps), min(count, count - steps))
    return lax.ppermute(value, axis, [(source, source + steps) for source in range(first, last)])


def entering(shard, axis, join, neutral):
    place = lax.axis_index(axis)
    gathered = jax.tree.map(
        lambda a, kind: lax.all_gather(a.astype(kind), axis), shard, (jnp.bfloat16, jnp.bfloat16)
    )
    state = jax.tree.map(lambda a, e: jnp.zeros_like(a) + jnp.asarray(e, a.dtype), shard, neutral)

    def one(step, state):
        return join(
            state,
            jax.tree.map(
                lambda a, own: lax.dynamic_index_in_dim(a, step, 0, False).astype(own.dtype),
                gathered,
                shard,
            ),
        )

    return lax.fori_loop(0, place, one, state)


def rms_scale(values, gain):
    return values * lax.rsqrt(jnp.mean(values * values, axis=-1, keepdims=True) + EPSILON) * gain


def join_state(earlier, later):
    decay_one, state_one = earlier
    decay_two, state_two = later
    return (decay_one * decay_two, decay_two[..., None] * state_one + state_two)


def swapped(value, axis, bits):
    count = lax.axis_size(axis)
    return lax.ppermute(value, axis, [(source, source ^ bits) for source in range(count)])


def picked(stack, place, axis=0):
    return lax.dynamic_index_in_dim(stack, place, axis, False)


def halves_divide(tokens, query_weight, pooling_input_weight, pooling_group_maps, decay_spike, out_weight):
    planes, members, cores = (lax.axis_size(axis) for axis in ("sp", "fs", "tp"))
    heads = decay_spike.shape[2]
    width = query_weight.shape[1] // heads
    return (
        cores == 2
        and planes == 2 * cores
        and members == 2 * cores
        and heads == 2 * cores
        and width % 128 == 0
        and pooling_group_maps.shape[0] * 2 == heads
        and pooling_input_weight.shape[1] == query_weight.shape[1]
        and tokens.shape[0] == 1
        and tokens.shape[1] % BLOCK == 0
        and decay_spike.shape[1] == cores * tokens.shape[1] == width
        and query_weight.shape[0] == heads * width
        and out_weight.shape[1] == heads * width
        and pooling_group_maps.shape[1] == 2 * width
        and 2 ** (2 * pooling_group_maps.shape[0]) <= HALO
    )


HALO = 16
MEBI = 2**20


def places():
    plane, member, core = (lax.axis_index(axis) for axis in ("sp", "fs", "tp"))
    late, half = lax.div(plane, 2), lax.rem(plane, 2)
    row, side = lax.div(member, 2), lax.rem(member, 2)
    return plane, late, half, row, side, core


def first_kernel(width, rows_each, *refs):
    sources, inputs, messages, rows_out = refs[:3], refs[3:7], refs[7:9], refs[9]
    locals_in, sems = refs[10:13], refs[13]
    tokens, gain, spikes = locals_in
    _, _, half, row, side, core = places()
    loads = [
        pltpu.make_async_copy(source, target, sems.at[8 + n])
        for n, (source, target) in enumerate(zip(sources, locals_in))
    ]
    for copy in loads:
        copy.start()
    part = inputs[0].shape[0] // 2
    top = pl.multiple_of(side * part, part)
    first = jnp.where(core == half, 0, 1)
    copies = []
    for n in range(2):
        place = 2 * row + jnp.where(n == 0, first, 1 - first)
        column = pl.multiple_of(place * width, width)
        for m, w in enumerate(inputs):
            copies.append(
                pltpu.make_async_copy(
                    w.at[pl.ds(top, part), pl.ds(column, width)],
                    messages[n].at[:, pl.ds(m * width, width)],
                    sems.at[n * 4 + m],
                )
            )
    for copy in copies:
        copy.start()
    for copy in loads:
        copy.wait()
    values = tokens[...].astype(jnp.float32)
    rows_out[pl.ds(0, rows_each), :] = rms_scale(values, gain[...]).astype(jnp.bfloat16)
    rows_out[pl.ds(rows_each, 8), :] = jnp.zeros((8, rows_out.shape[1]), jnp.bfloat16)
    upper = spikes[...].astype(jnp.bfloat16)
    lower = (spikes[...] - upper.astype(jnp.float32)).astype(jnp.bfloat16)
    rows_out[pl.ds(rows_each, 8), pl.ds(0, width)] = jnp.concatenate([upper, lower], axis=0)
    for copy in copies:
        copy.wait()


def pack_kernel(width, *refs):
    sources = refs[:3]
    inputs, maps, pool_weight, rec_weight = refs[3:7], refs[7], refs[8], refs[9]
    messages, blocks, own_vectors, partner_vectors, pooled = refs[10:12], refs[12:14], *refs[14:17]
    group_map, group_rows, scale, bound, head_gain, sems = refs[17:]
    _, _, half, row, _, core = places()
    rows = inputs[0].shape[0]
    size = maps.shape[1]
    begin = pl.multiple_of(row * size, size)
    first = jnp.where(core == half, 0, 1)
    group_copies = [
        pltpu.make_async_copy(maps.at[row], group_map, sems.at[0]),
        pltpu.make_async_copy(pool_weight.at[pl.ds(begin, size), :], group_rows, sems.at[1]),
    ]
    group_copies += [
        pltpu.make_async_copy(source, target, sems.at[14 + n])
        for n, (source, target) in enumerate(zip(sources, (scale, bound, head_gain)))
    ]
    copies = []
    targets = []
    for n, place in enumerate((1 - core, core)):
        column = pl.multiple_of((2 * row + place) * width, width)
        copies += [
            pltpu.make_async_copy(
                w.at[:, pl.ds(column, width)],
                blocks[n].at[pl.ds(0, rows), pl.ds(m * width, width)],
                sems.at[2 + 4 * n + m],
            )
            for m, w in enumerate(inputs)
        ]
        targets.append((place, blocks[n].at[pl.ds(rows + width, width), :]))
    for n in range(2):
        place = jnp.where(n == 0, first, 1 - first)
        targets.append((place, messages[n].at[pl.ds(width, width), :]))
    for n, (place, target) in enumerate(targets):
        at = pl.ds(pl.multiple_of((2 * row + place) * width, width), width)
        copies.append(pltpu.make_async_copy(rec_weight.at[at, :], target, sems.at[10 + n]))
    for copy in group_copies + copies:
        copy.start()
    for copy in group_copies:
        copy.wait()
    for place, target in ((2 * row + core, own_vectors), (2 * row + 1 - core, partner_vectors)):
        at = pl.ds(pl.multiple_of(place * width, width), width)
        for n, vector in enumerate((bound, head_gain)):
            target[pl.ds(n, 1), :] = vector[:, at]
    scaled = group_map[...].astype(jnp.float32) * scale[:, pl.ds(begin, size)]
    high = scaled.astype(jnp.bfloat16)
    rest = (scaled - high.astype(jnp.float32)).astype(jnp.bfloat16)
    pooled[...] = (
        jnp.dot(high, group_rows[...], preferred_element_type=jnp.float32)
        + jnp.dot(rest, group_rows[...], preferred_element_type=jnp.float32)
    ).astype(jnp.bfloat16)
    for block, place in zip(blocks, (1 - core, core)):
        block[pl.ds(rows, width), :] = pooled[pl.ds(pl.multiple_of(place * width, width), width), :]
    for n in range(2):
        place = jnp.where(n == 0, first, 1 - first)
        messages[n][pl.ds(0, width), :] = pooled[
            pl.ds(pl.multiple_of(place * width, width), width), :
        ]
    for copy in copies:
        copy.wait()


def down(values, steps):
    rows = lax.broadcasted_iota(jnp.int32, values.shape, 0)
    return jnp.where(rows >= steps, pltpu.roll(values, steps, 0), 0.0)


def start_pieces(pieces, blocks, sems, plane, core, owns, put):
    planes = lax.axis_size("sp")
    near, far, last = (
        lax.rem(plane + k, planes) for k in (2 - core, 1 + core, 3)
    )
    waits = []
    used = 0

    def copies(group, source, slot):
        return [
            pltpu.make_async_copy(piece, put(source, n), sems.at[slot + n])
            for n, piece in enumerate(group)
        ]

    for group, source in zip(pieces[:2], (near, far)):
        made = copies(group, source, used)
        for copy in made:
            copy.start()
        waits += made
        used += len(group)
    choices = [copies(group, last, used) for group in pieces[2:]]
    for n in range(2):

        @pl.when(core == n)
        def _(n=n):
            for copy in choices[n]:
                copy.start()

    waits += choices[0]
    used += len(choices[0])
    for n, group in enumerate(blocks):
        for m, (source, target) in enumerate(group):
            copy = pltpu.make_async_copy(source, target, sems.at[used + m])

            @pl.when(owns if n == 0 else jnp.logical_not(owns))
            def _(copy=copy):
                copy.start()

            if n == 0:
                waits.append(copy)
    return waits


def state_kernel(width, rows_each, *refs):
    own_vectors, partner_vectors = refs[:2]
    tokens, pieces, blocks = refs[2:10], refs[10:18], refs[18:20]
    read_local, read_full, pool_rows, carry = refs[20:24]
    token_all, weight_in, spikes, token_sems, sems = refs[24:]
    plane, _, half, row, side, core = places()
    owns = core == half
    column = 2 * row + core
    plane_rows = 4 * width
    part = plane_rows // 2
    waits = []
    used = 0
    for a in range(2):
        for b in range(2):
            for c in range(2):
                piece = tokens[(a * 2 + b) * 2 + c]
                order = ((row ^ b) * 2 + (half ^ a)) * 2 + (core ^ c)
                top = pl.multiple_of(order * rows_each, rows_each)
                waits.append(
                    pltpu.make_async_copy(
                        piece.at[pl.ds(0, rows_each), :],
                        token_all.at[pl.ds(top, rows_each), :],
                        token_sems.at[used],
                    )
                )
                waits.append(
                    pltpu.make_async_copy(
                        piece.at[pl.ds(rows_each, 8), pl.ds(0, width)],
                        spikes.at[order],
                        token_sems.at[used + 1],
                    )
                )
                used += 2
    for copy in waits:
        copy.start()

    def put(source, n):
        x = side if n == 0 else 1 - side
        return weight_in.at[pl.ds(pl.multiple_of(source * plane_rows + x * part, part), part), :]

    begin = pl.ds(pl.multiple_of(plane * plane_rows, plane_rows), plane_rows)
    ends = [[(block.at[pl.ds(0, plane_rows), :], weight_in.at[begin, :])] for block in blocks]
    pairs = [pieces[2 * n : 2 * n + 2] for n in range(4)]
    more = start_pieces(pairs, ends, sems, plane, core, owns, put)
    for copy in waits + more:
        copy.wait()
    lower_bound = jnp.where(owns, own_vectors[pl.ds(0, 1), :], partner_vectors[pl.ds(0, 1), :])
    projected = jnp.dot(token_all[...], weight_in[...], preferred_element_type=jnp.float32)
    projected = projected.astype(jnp.bfloat16)
    pool_rows[...] = projected[:, :width]
    query, forget_logit, value = (
        projected[:, n * width : (n + 1) * width].astype(jnp.float32) for n in range(1, 4)
    )
    spike_row = lax.broadcasted_iota(jnp.int32, (8, width), 0)
    wanted_row = jnp.logical_or(spike_row == column, spike_row == column + 4)
    spike_columns = []
    for n in range(4):
        parts = spikes[2 * n + half].astype(jnp.float32)
        line = jnp.sum(jnp.where(wanted_row, parts, 0.0), axis=0, keepdims=True)
        spike_columns.append(jnp.broadcast_to(line, (width, width)).T)
    spike = jnp.concatenate(spike_columns, axis=0)
    reader = query * jax.nn.sigmoid(query)
    key_gate = jax.nn.sigmoid(-lower_bound) * jax.nn.sigmoid(-forget_logit)
    log_decay = jnp.log1p(-key_gate) + spike
    t_at = lax.broadcasted_iota(jnp.int32, (BLOCK, BLOCK), 0)
    s_at = lax.broadcasted_iota(jnp.int32, (BLOCK, BLOCK), 1)
    causal = t_at >= s_at
    lower = causal.astype(jnp.float32)
    length = 4 * rows_each
    states = [jnp.zeros((width, width), jnp.float32)] * 2
    before = [jnp.zeros((1, width), jnp.float32)] * 2
    for n in range(length // BLOCK):
        for seq in range(2):
            begin = seq * length + n * BLOCK
            rows = slice(begin, begin + BLOCK)
            inner_log = jnp.dot(
                lower, log_decay[rows], preferred_element_type=jnp.float32, precision=HIGHEST
            )
            keys = key_gate[rows]
            values = value[rows].astype(jnp.bfloat16)
            grown = reader[rows] * jnp.exp(inner_log)
            read_scaled = grown.astype(jnp.bfloat16)
            key_scaled = (keys * jnp.exp(-inner_log)).astype(jnp.bfloat16)
            scores = lax.dot_general(
                read_scaled, key_scaled, (((1,), (1,)), ((), ())), preferred_element_type=jnp.float32
            )
            scores = jnp.where(causal, scores, 0.0).astype(jnp.bfloat16)
            read = jnp.dot(scores, values, preferred_element_type=jnp.float32)
            if n > 0:
                read = read + jnp.dot(
                    read_scaled,
                    states[seq].astype(jnp.bfloat16),
                    preferred_element_type=jnp.float32,
                )
            closing = inner_log[BLOCK - 1 : BLOCK]
            key_tail = (keys * jnp.exp(closing - inner_log)).astype(jnp.bfloat16)
            added = lax.dot_general(
                key_tail, values, (((0,), (0,)), ((), ())), preferred_element_type=jnp.float32
            )
            share = jnp.broadcast_to(jnp.exp(closing), (width, width)).T
            states[seq] = share * states[seq] + added
            read_local[pl.ds(begin, BLOCK), :] = read
            read_full[pl.ds(begin, BLOCK), :] = (grown * jnp.exp(before[seq])).astype(jnp.bfloat16)
            before[seq] = before[seq] + closing
    for seq in range(2):
        top = seq * (width + HALO)
        carry[pl.ds(top, width), :] = states[seq].astype(jnp.bfloat16)
        carry[pl.ds(top + width, HALO), :] = projected[
            (seq + 1) * length - HALO : (seq + 1) * length, :width
        ]


def output_kernel(width, rows_each, *refs):
    own_vectors, partner_vectors, read_local, read_full, pool_rows, carry = refs[:6]
    pieces, blocks = refs[6:10], refs[10:12]
    sent, kept = refs[12:14]
    weight_out, mixed, sems = refs[14:]
    plane, late, half, row, _, core = places()
    owns = core == half
    plane_rows = 4 * width
    length = 4 * rows_each

    def put(source, n):
        return weight_out.at[source]

    ends = [[(block.at[pl.ds(plane_rows, 2 * width), :], weight_out.at[plane])] for block in blocks]
    singles = [[piece] for piece in pieces]
    waits = start_pieces(singles, ends, sems, plane, core, owns, put)
    head_gain = jnp.where(owns, own_vectors[pl.ds(1, 1), :], partner_vectors[pl.ds(1, 1), :])
    group = 2 * half + row
    window = jnp.left_shift(jnp.int32(2), group)
    for seq in range(2):
        top = seq * (width + HALO)
        rows = pl.ds(seq * length, length)
        extended = jnp.concatenate(
            [carry[pl.ds(top + width, HALO), :], pool_rows[rows, :]], axis=0
        ).astype(jnp.float32)
        window_sum = extended
        chosen = jnp.zeros_like(extended)
        for g in range(4):
            window_sum = window_sum + down(window_sum, 2**g)
            chosen = jnp.where(group == g, window_sum, chosen)
        at = lax.broadcasted_iota(jnp.int32, (length, width), 0) + late * length
        counts = jnp.minimum(at + 1, window).astype(jnp.float32)
        mixed[rows, pl.ds(0, width)] = (chosen[HALO:] / counts - extended[HALO:]).astype(
            jnp.bfloat16
        )
        read = read_local[rows, :] + jnp.dot(
            read_full[rows, :], carry[pl.ds(top, width), :], preferred_element_type=jnp.float32
        )
        mixed[rows, pl.ds(width, width)] = (rms_scale(read, 1.0) * head_gain).astype(jnp.bfloat16)
    for copy in waits:
        copy.wait()
    for target, c in ((sent, 1 - core), (kept, core)):
        for n in range(4):
            top = pl.multiple_of((n * 2 + c) * rows_each, rows_each)
            rows = mixed[pl.ds(top, rows_each), :]
            for p in range(weight_out.shape[0]):
                target[n // 2, n % 2, :, pl.ds(p * plane_rows, plane_rows)] = jnp.dot(
                    rows, weight_out[p], preferred_element_type=jnp.float32
                ).astype(jnp.bfloat16)


def by_halves(
    tokens,
    input_norm_gain,
    pooling_input_weight,
    query_weight,
    forget_weight,
    value_weight,
    pooling_group_maps,
    pooling_scale,
    lower_bound_logits,
    decay_spike,
    head_norm_gain,
    pooling_output_weight,
    recurrent_output_weight,
):
    planes, members, cores = (lax.axis_size(axis) for axis in ("sp", "fs", "tp"))
    _, _, half, row, _, _ = places()
    heads = decay_spike.shape[2]
    width = query_weight.shape[1] // heads
    features = tokens.shape[2]
    rows_each = tokens.shape[1]
    part = query_weight.shape[0] // 2
    hbm = pl.BlockSpec(memory_space=pltpu.HBM)
    vmem = pl.BlockSpec(memory_space=pltpu.VMEM)

    def made(*shape, kind=jnp.bfloat16):
        return pltpu.VMEM(shape, kind)

    def near(*values):
        return [pltpu.with_memory_space_constraint(v, pltpu.VMEM) for v in values]

    def pack(*refs):
        pack_kernel(width, *refs)

    def far(*values):
        return [pltpu.with_memory_space_constraint(v, pltpu.HBM) for v in values]

    weights_in = far(pooling_input_weight, query_weight, forget_weight, value_weight)

    def first(*refs):
        first_kernel(width, rows_each, *refs)

    *messages, own_rows = pl.pallas_call(
        first,
        out_shape=[made(part, 4 * width)] * 2 + [made(rows_each + 8, features)],
        in_specs=[hbm] * 7,
        out_specs=[vmem] * 3,
        scratch_shapes=[
            pltpu.VMEM((rows_each, features), jnp.bfloat16),
            pltpu.VMEM((1, features), jnp.float32),
            pltpu.VMEM((heads, width), jnp.float32),
            pltpu.SemaphoreType.DMA((11,)),
        ],
        compiler_params=pltpu.CompilerParams(vmem_limit_bytes=8 * MEBI),
        name="first",
    )(*far(tokens[0], input_norm_gain[None], decay_spike[0].T), *weights_in)
    *out_messages, partner_block, own_block, vectors, partner_vectors, _ = pl.pallas_call(
        pack,
        out_shape=[made(2 * width, 4 * width)] * 2
        + [made(2 * part + 2 * width, 4 * width)] * 2
        + [made(2, width, kind=jnp.float32)] * 2
        + [made(2 * width, 4 * width)],
        in_specs=[hbm] * 10,
        out_specs=[vmem] * 7,
        scratch_shapes=[
            pltpu.VMEM(pooling_group_maps.shape[1:], jnp.bfloat16),
            pltpu.VMEM((2 * width, 4 * width), jnp.bfloat16),
        ]
        + [pltpu.VMEM((1, heads * width), jnp.float32)] * 3
        + [
            pltpu.SemaphoreType.DMA((17,)),
        ],
        compiler_params=pltpu.CompilerParams(vmem_limit_bytes=12 * MEBI),
        name="pack",
    )(
        *far(pooling_scale[None], lower_bound_logits[None], head_norm_gain[None]),
        *weights_in,
        *far(pooling_group_maps, pooling_output_weight, recurrent_output_weight),
    )

    def hops(wanted):
        return [
            (((p + k) % planes) * cores + p % cores, p * cores + c)
            for p in range(planes)
            for k, c in wanted
        ]

    rounds = (
        (0, hops([(2, 0), (1, 1)])),
        (1, hops([(2, 1), (1, 0)])),
        (1, hops([(3, 0)])),
        (0, hops([(3, 1)])),
    )

    def shared(pair):
        pieces = []
        for n, (which, pairs) in enumerate(rounds):
            arrived = lax.ppermute(pair[which], ("sp", "tp"), pairs)
            pieces.append(arrived)
            used = range(cores) if n < 2 else (n - 2,)
            across = [(f * cores + c, (f ^ 1) * cores + c) for f in range(members) for c in used]
            pieces.append(lax.ppermute(arrived, ("fs", "tp"), across))
        return pieces

    pieces = shared(messages)
    output_pieces = []
    for which, pairs in rounds:
        output_pieces.append(lax.ppermute(out_messages[which], ("sp", "tp"), pairs))
    partner_local = swapped(partner_block, "tp", 1)

    received_vectors = swapped(partner_vectors, "tp", 1)
    other_rows = swapped(own_rows, "sp", 1)
    chip_rows = []
    for rows in (own_rows, other_rows):
        chip_rows += [rows, swapped(rows, "fs", 2)]
    token_pieces = []
    for rows in chip_rows:
        token_pieces += [rows, swapped(rows, "tp", 1)]

    length = 8 * rows_each
    carry_shape = made(2 * (width + HALO), width)

    def state(*refs):
        state_kernel(width, rows_each, *refs)

    read_local, read_full, pool_rows, carry = pl.pallas_call(
        state,
        out_shape=[
            made(length, width, kind=jnp.float32),
            made(length, width),
            made(length, width),
            carry_shape,
        ],
        in_specs=[vmem] * 20,
        out_specs=[vmem] * 4,
        scratch_shapes=[
            pltpu.VMEM((length, features), jnp.bfloat16),
            pltpu.VMEM((features, 4 * width), jnp.bfloat16),
            pltpu.VMEM((8, 8, width), jnp.bfloat16),
            pltpu.SemaphoreType.DMA((16,)),
            pltpu.SemaphoreType.DMA((7,)),
        ],
        compiler_params=pltpu.CompilerParams(vmem_limit_bytes=24 * MEBI),
        name="state",
    )(
        *near(vectors, received_vectors, *token_pieces, *pieces, own_block, partner_local),
    )
    entering_carry = lax.ppermute(carry, "sp", [(p, p + 2) for p in range(planes - 2)])

    def output(*refs):
        output_kernel(width, rows_each, *refs)

    half_shape = made(2, 2, rows_each, features)
    sent, kept = pl.pallas_call(
        output,
        out_shape=[half_shape] * 2,
        in_specs=[vmem] * 12,
        out_specs=[vmem] * 2,
        scratch_shapes=[
            pltpu.VMEM((planes, 2 * width, 4 * width), jnp.bfloat16),
            pltpu.VMEM((length, 2 * width), jnp.bfloat16),
            pltpu.SemaphoreType.DMA((4,)),
        ],
        compiler_params=pltpu.CompilerParams(vmem_limit_bytes=20 * MEBI),
        name="output",
    )(
        *near(vectors, received_vectors, read_local, read_full, pool_rows, entering_carry),
        *near(*output_pieces, own_block, partner_local),
    )
    from_partner = swapped(sent, "tp", 1)
    middle = features // 2

    def joined(place, axis, columns):
        return sum(
            picked(v[..., columns], place, axis).astype(jnp.float32) for v in (kept, from_partner)
        )

    left, right = slice(0, middle), slice(middle, features)
    left_in = swapped(joined(1 - row, 0, left).astype(jnp.bfloat16), "fs", 2)
    right_in = swapped(joined(1 - half, 1, right).astype(jnp.bfloat16), "sp", 1)
    left_sum = joined(row, 0, left) + left_in.astype(jnp.float32)
    right_sum = joined(half, 1, right) + right_in.astype(jnp.float32)
    left_last = swapped(picked(left_sum, 1 - half).astype(jnp.bfloat16), "sp", 1)
    right_last = swapped(picked(right_sum, 1 - row).astype(jnp.bfloat16), "fs", 2)
    left_total = picked(left_sum, half) + left_last.astype(jnp.float32)
    right_total = picked(right_sum, row) + right_last.astype(jnp.float32)
    total = jnp.concatenate([left_total, right_total], axis=1)
    return total.astype(jnp.bfloat16)[None]


def body(*arrays):
    tokens, _, pool_in, query_in, _, _, maps, _, _, spike, _, pool_out, _ = arrays
    if halves_divide(tokens, query_in, pool_in, maps, spike, pool_out):
        return by_halves(*arrays)
    return by_positions(*arrays)


def by_positions(
    tokens,
    input_norm_gain,
    pooling_input_weight,
    query_weight,
    forget_weight,
    value_weight,
    pooling_group_maps,
    pooling_scale,
    lower_bound_logits,
    decay_spike,
    head_norm_gain,
    pooling_output_weight,
    recurrent_output_weight,
):
    gathered = lax.all_gather(tokens, "tp", axis=1, tiled=True)[0]
    length_total = gathered.shape[0]
    normed = rms_scale(gathered.astype(jnp.float32), input_norm_gain).astype(jnp.bfloat16)
    pool_width = pooling_input_weight.shape[1]
    rec_width = query_weight.shape[1]
    stacked = jnp.concatenate(
        [pooling_input_weight, query_weight, forget_weight, value_weight], axis=1
    )
    out_local = jnp.concatenate([pooling_output_weight, recurrent_output_weight], axis=0)
    groups_fs = lax.axis_size("fs")
    member = lax.axis_index("fs")
    slice_width = stacked.shape[1] // groups_fs
    own_slice = lax.dynamic_slice_in_dim(stacked, member * slice_width, slice_width, 1)
    column_part = lax.all_gather(own_slice, "sp", axis=0, tiled=True)
    full_input = lax.all_gather(column_part, "fs", axis=1, tiled=True)
    projected = jnp.dot(normed, full_input, preferred_element_type=jnp.float32)
    slice_height = out_local.shape[0] // groups_fs
    own_rows = lax.dynamic_slice_in_dim(out_local, member * slice_height, slice_height, 0)
    row_part = lax.all_gather(own_rows, "sp", axis=1, tiled=True)
    out_full = lax.all_gather(row_part, "fs", axis=0, tiled=True)
    rounded = lax.optimization_barrier(projected.astype(jnp.bfloat16))
    pool_input = rounded[:, :pool_width]
    query_matrix = rounded[:, pool_width : pool_width + rec_width].astype(jnp.float32)
    forget_gate_logit = rounded[:, pool_width + rec_width : pool_width + 2 * rec_width].astype(
        jnp.float32
    )
    value_projected = rounded[:, pool_width + 2 * rec_width :].astype(jnp.float32)
    groups_local = pooling_group_maps.shape[0]
    group_size = pooling_group_maps.shape[1]
    reach_rows = 2 ** (groups_local * lax.axis_size("tp"))
    previous = shifted(pool_input[length_total - reach_rows :], "sp", 1)
    extended = jnp.concatenate([previous, pool_input], axis=0).astype(jnp.float32)
    extended = extended.reshape(reach_rows + length_total, groups_local, group_size)
    group_ids = lax.axis_index("tp") * groups_local + jnp.arange(groups_local, dtype=jnp.int32)
    windows = jnp.left_shift(jnp.int32(2), group_ids)
    window_sum = jnp.zeros((length_total, groups_local, group_size), jnp.float32)
    for offset in range(reach_rows):
        inside = (offset < windows).astype(jnp.float32)
        window_sum = (
            window_sum
            + extended[reach_rows - offset : reach_rows - offset + length_total] * inside[:, None]
        )
    position_index = lax.axis_index("sp") * length_total + jnp.arange(length_total, dtype=jnp.int32)
    counts = jnp.minimum(position_index[:, None] + 1, windows[None, :]).astype(jnp.float32)
    pool_diff = (window_sum / counts[:, :, None] - extended[reach_rows:]).astype(jnp.bfloat16)
    pool_mapped = jnp.einsum(
        "tgc,gcd->tgd", pool_diff, pooling_group_maps, preferred_element_type=jnp.float32
    )
    pool_out = (pool_mapped.reshape(length_total, pool_width) * pooling_scale).astype(jnp.bfloat16)
    local_heads = decay_spike.shape[2]
    head_width = rec_width // local_heads
    blocks = length_total // BLOCK
    block_layout = (blocks, BLOCK, local_heads, head_width)
    reader = jax.nn.silu(query_matrix).reshape(block_layout)
    key_gate_value = jax.nn.sigmoid(-lower_bound_logits) * jax.nn.sigmoid(-forget_gate_logit)
    decay_logarithm = (
        jnp.log1p(-key_gate_value).reshape(length_total, local_heads, head_width)
        + decay_spike[0][:, :, None]
    ).reshape(block_layout)
    key_rows = key_gate_value.reshape(block_layout)
    value_rows = value_projected.reshape(block_layout)
    inner_log = jnp.cumsum(decay_logarithm, axis=1)
    read_scaled = reader * jnp.exp(inner_log)
    key_scaled = key_rows * jnp.exp(-inner_log)
    causal = (jnp.arange(BLOCK)[:, None] >= jnp.arange(BLOCK)[None, :]).astype(jnp.float32)
    scores = jnp.einsum("nthd,nshd->nhts", read_scaled, key_scaled, precision=HIGHEST) * causal
    within = jnp.einsum("nhts,nshe->nthe", scores, value_rows, precision=HIGHEST)
    closing = inner_log[:, -1]
    key_tail = key_rows * jnp.exp(closing[:, None] - inner_log)
    deltas = jnp.einsum("nshd,nshe->nhde", key_tail, value_rows, precision=HIGHEST)
    block_decay = jnp.exp(closing)

    def advance(carried, input_batch):
        decay_now, delta_now = input_batch
        return (decay_now[..., None] * carried + delta_now, carried)

    initial = jnp.zeros((local_heads, head_width, head_width), jnp.float32)
    device_state, entry_states = lax.scan(advance, initial, (block_decay, deltas))
    device_decay = jnp.exp(jnp.sum(closing, axis=0))
    scanned = entering(
        (device_decay, device_state),
        "sp",
        join_state,
        (jnp.ones_like(device_decay), jnp.zeros_like(device_state)),
    )
    prior_state = scanned[1]
    before = jnp.cumsum(closing, axis=0) - closing
    start_states = entry_states + jnp.exp(before)[..., None] * prior_state[None]
    read_out = within + jnp.einsum("nthd,nhde->nthe", read_scaled, start_states, precision=HIGHEST)
    read_out = read_out.reshape(length_total, local_heads, head_width)
    recurrent_output = (
        rms_scale(read_out, 1.0).reshape(length_total, rec_width) * head_norm_gain
    ).astype(jnp.bfloat16)
    mixed_rows = jnp.concatenate([pool_out, recurrent_output], axis=1)
    summed = lax.psum_scatter(
        jnp.dot(mixed_rows, out_full, preferred_element_type=jnp.float32).astype(jnp.bfloat16),
        "tp",
        scatter_dimension=0,
        tiled=True,
    )
    return summed[None]


def solution(mesh):
    placed = (
        P("fs", ("sp", "tp"), None),
        P(),
        P("sp", "tp"),
        P("sp", "tp"),
        P("sp", "tp"),
        P("sp", "tp"),
        P("tp", None, None),
        P("tp"),
        P("tp"),
        P("fs", "sp", "tp"),
        P("tp"),
        P("tp", "sp"),
        P("tp", "sp"),
    )
    return jax.shard_map(
        body, mesh=mesh, in_specs=placed, out_specs=P("fs", ("sp", "tp"), None), check_vma=False
    )
```

```python
import jax
import jax.numpy as jnp
from jax import lax
from jax.experimental import pallas as pl
from jax.experimental.pallas import tpu as pltpu
from jax.sharding import PartitionSpec as P

BLOCK = 64


EPSILON = 1e-06
HIGHEST = lax.Precision.HIGHEST


def shifted(value, axis, steps):
    count = lax.axis_size(axis)
    first, last = (max(0, -steps), min(count, count - steps))
    return lax.ppermute(value, axis, [(source, source + steps) for source in range(first, last)])


def entering(shard, axis, join, neutral):
    place = lax.axis_index(axis)
    gathered = jax.tree.map(
        lambda a, kind: lax.all_gather(a.astype(kind), axis), shard, (jnp.bfloat16, jnp.bfloat16)
    )
    state = jax.tree.map(lambda a, e: jnp.zeros_like(a) + jnp.asarray(e, a.dtype), shard, neutral)

    def one(step, state):
        return join(
            state,
            jax.tree.map(
                lambda a, own: lax.dynamic_index_in_dim(a, step, 0, False).astype(own.dtype),
                gathered,
                shard,
            ),
        )

    return lax.fori_loop(0, place, one, state)


def rms_scale(values, gain):
    return values * lax.rsqrt(jnp.mean(values * values, axis=-1, keepdims=True) + EPSILON) * gain


def join_state(earlier, later):
    decay_one, state_one = earlier
    decay_two, state_two = later
    return (decay_one * decay_two, decay_two[..., None] * state_one + state_two)


def swapped(value, axis, bits):
    count = lax.axis_size(axis)
    return lax.ppermute(value, axis, [(source, source ^ bits) for source in range(count)])


def picked(stack, place, axis=0):
    return lax.dynamic_index_in_dim(stack, place, axis, False)


def halves_divide(tokens, query_weight, pooling_input_weight, pooling_group_maps, decay_spike, out_weight):
    planes, members, cores = (lax.axis_size(axis) for axis in ("sp", "fs", "tp"))
    heads = decay_spike.shape[2]
    width = query_weight.shape[1] // heads
    return (
        cores == 2
        and planes == 2 * cores
        and members == 2 * cores
        and heads == 2 * cores
        and width % 128 == 0
        and pooling_group_maps.shape[0] * 2 == heads
        and pooling_input_weight.shape[1] == query_weight.shape[1]
        and tokens.shape[0] == 1
        and tokens.shape[1] % BLOCK == 0
        and decay_spike.shape[1] == cores * tokens.shape[1] == width
        and query_weight.shape[0] == heads * width
        and out_weight.shape[1] == heads * width
        and pooling_group_maps.shape[1] == 2 * width
        and 2 ** (2 * pooling_group_maps.shape[0]) <= HALO
    )


HALO = 16
MEBI = 2**20


def places():
    plane, member, core = (lax.axis_index(axis) for axis in ("sp", "fs", "tp"))
    late, half = lax.div(plane, 2), lax.rem(plane, 2)
    row, side = lax.div(member, 2), lax.rem(member, 2)
    return plane, late, half, row, side, core


def first_kernel(width, rows_each, *refs):
    sources, inputs, messages, rows_out = refs[:3], refs[3:7], refs[7:9], refs[9]
    locals_in, sems = refs[10:13], refs[13]
    tokens, gain, spikes = locals_in
    _, _, half, row, side, core = places()
    loads = [
        pltpu.make_async_copy(source, target, sems.at[8 + n])
        for n, (source, target) in enumerate(zip(sources, locals_in))
    ]
    for copy in loads:
        copy.start()
    part = inputs[0].shape[0] // 2
    top = pl.multiple_of(side * part, part)
    first = jnp.where(core == half, 0, 1)
    copies = []
    for n in range(2):
        place = 2 * row + jnp.where(n == 0, first, 1 - first)
        column = pl.multiple_of(place * width, width)
        for m, w in enumerate(inputs):
            copies.append(
                pltpu.make_async_copy(
                    w.at[pl.ds(top, part), pl.ds(column, width)],
                    messages[n].at[:, pl.ds(m * width, width)],
                    sems.at[n * 4 + m],
                )
            )
    for copy in copies:
        copy.start()
    for copy in loads:
        copy.wait()
    values = tokens[...].astype(jnp.float32)
    rows_out[pl.ds(0, rows_each), :] = rms_scale(values, gain[...]).astype(jnp.bfloat16)
    rows_out[pl.ds(rows_each, 8), :] = jnp.zeros((8, rows_out.shape[1]), jnp.bfloat16)
    upper = spikes[...].astype(jnp.bfloat16)
    lower = (spikes[...] - upper.astype(jnp.float32)).astype(jnp.bfloat16)
    rows_out[pl.ds(rows_each, 8), pl.ds(0, width)] = jnp.concatenate([upper, lower], axis=0)
    for copy in copies:
        copy.wait()


def pack_kernel(width, *refs):
    sources = refs[:3]
    inputs, maps, pool_weight, rec_weight = refs[3:7], refs[7], refs[8], refs[9]
    messages, blocks, own_vectors, partner_vectors, pooled = refs[10:12], refs[12:14], *refs[14:17]
    group_map, group_rows, scale, bound, head_gain, sems = refs[17:]
    _, _, half, row, side, core = places()
    rows = inputs[0].shape[0]
    size = maps.shape[1]
    begin = pl.multiple_of(row * size, size)
    first = jnp.where(core == half, 0, 1)
    group_copies = [
        pltpu.make_async_copy(maps.at[row], group_map, sems.at[0]),
        pltpu.make_async_copy(pool_weight.at[pl.ds(begin, size), :], group_rows, sems.at[1]),
    ]
    group_copies += [
        pltpu.make_async_copy(source, target, sems.at[14 + n])
        for n, (source, target) in enumerate(zip(sources, (scale, bound, head_gain)))
    ]
    copies = []
    targets = []
    top = pl.ds(pl.multiple_of(side * (rows // 2), rows // 2), rows // 2)
    for n, place in enumerate((1 - core, core)):
        column = pl.multiple_of((2 * row + place) * width, width)
        copies += [
            pltpu.make_async_copy(
                w.at[:, pl.ds(column, width)],
                blocks[n].at[pl.ds(0, rows), pl.ds(m * width, width)],
                sems.at[2 + 4 * n + m],
            )
            for m, w in enumerate(inputs)
        ]
        targets.append((place, slice(None), blocks[n].at[pl.ds(rows + width, width), :]))
    for n in range(2):
        place = jnp.where(n == 0, first, 1 - first)
        targets.append((place, top, messages[n].at[pl.ds(width, width), :]))
    for n, (place, columns, target) in enumerate(targets):
        at = pl.ds(pl.multiple_of((2 * row + place) * width, width), width)
        copies.append(pltpu.make_async_copy(rec_weight.at[at, columns], target, sems.at[10 + n]))
    for copy in group_copies + copies:
        copy.start()
    for copy in group_copies:
        copy.wait()
    for place, target in ((2 * row + core, own_vectors), (2 * row + 1 - core, partner_vectors)):
        at = pl.ds(pl.multiple_of(place * width, width), width)
        for n, vector in enumerate((bound, head_gain)):
            target[pl.ds(n, 1), :] = vector[:, at]
    scaled = group_map[...].astype(jnp.float32) * scale[:, pl.ds(begin, size)]
    high = scaled.astype(jnp.bfloat16)
    rest = (scaled - high.astype(jnp.float32)).astype(jnp.bfloat16)
    pooled[...] = (
        jnp.dot(high, group_rows[...], preferred_element_type=jnp.float32)
        + jnp.dot(rest, group_rows[...], preferred_element_type=jnp.float32)
    ).astype(jnp.bfloat16)
    for block, place in zip(blocks, (1 - core, core)):
        block[pl.ds(rows, width), :] = pooled[pl.ds(pl.multiple_of(place * width, width), width), :]
    for n in range(2):
        place = jnp.where(n == 0, first, 1 - first)
        messages[n][pl.ds(0, width), :] = pooled[
            pl.ds(pl.multiple_of(place * width, width), width), top
        ]
    for copy in copies:
        copy.wait()


def down(values, steps):
    rows = lax.broadcasted_iota(jnp.int32, values.shape, 0)
    return jnp.where(rows >= steps, pltpu.roll(values, steps, 0), 0.0)


def start_pieces(pieces, blocks, sems, plane, core, owns, put):
    planes = lax.axis_size("sp")
    near, far, last = (
        lax.rem(plane + k, planes) for k in (2 - core, 1 + core, 3)
    )
    waits = []
    used = 0

    def copies(group, source, slot):
        return [
            pltpu.make_async_copy(piece, put(source, n), sems.at[slot + n])
            for n, piece in enumerate(group)
        ]

    for group, source in zip(pieces[:2], (near, far)):
        made = copies(group, source, used)
        for copy in made:
            copy.start()
        waits += made
        used += len(group)
    choices = [copies(group, last, used) for group in pieces[2:]]
    for n in range(2):

        @pl.when(core == n)
        def _(n=n):
            for copy in choices[n]:
                copy.start()

    waits += choices[0]
    used += len(choices[0])
    for n, group in enumerate(blocks):
        for m, (source, target) in enumerate(group):
            copy = pltpu.make_async_copy(source, target, sems.at[used + m])

            @pl.when(owns if n == 0 else jnp.logical_not(owns))
            def _(copy=copy):
                copy.start()

            if n == 0:
                waits.append(copy)
    return waits


def state_kernel(width, rows_each, *refs):
    own_vectors, partner_vectors = refs[:2]
    tokens, pieces, blocks = refs[2:10], refs[10:18], refs[18:20]
    read_local, read_full, pool_rows, carry = refs[20:24]
    token_all, weight_in, spikes, token_sems, sems = refs[24:]
    plane, _, half, row, side, core = places()
    owns = core == half
    column = 2 * row + core
    plane_rows = 4 * width
    part = plane_rows // 2
    waits = []
    used = 0
    for a in range(2):
        for b in range(2):
            for c in range(2):
                piece = tokens[(a * 2 + b) * 2 + c]
                order = ((row ^ b) * 2 + (half ^ a)) * 2 + (core ^ c)
                top = pl.multiple_of(order * rows_each, rows_each)
                waits.append(
                    pltpu.make_async_copy(
                        piece.at[pl.ds(0, rows_each), :],
                        token_all.at[pl.ds(top, rows_each), :],
                        token_sems.at[used],
                    )
                )
                waits.append(
                    pltpu.make_async_copy(
                        piece.at[pl.ds(rows_each, 8), pl.ds(0, width)],
                        spikes.at[order],
                        token_sems.at[used + 1],
                    )
                )
                used += 2
    for copy in waits:
        copy.start()

    def put(source, n):
        x = side if n == 0 else 1 - side
        return weight_in.at[pl.ds(pl.multiple_of(source * plane_rows + x * part, part), part), :]

    begin = pl.ds(pl.multiple_of(plane * plane_rows, plane_rows), plane_rows)
    ends = [[(block.at[pl.ds(0, plane_rows), :], weight_in.at[begin, :])] for block in blocks]
    pairs = [pieces[2 * n : 2 * n + 2] for n in range(4)]
    more = start_pieces(pairs, ends, sems, plane, core, owns, put)
    for copy in waits + more:
        copy.wait()
    lower_bound = jnp.where(owns, own_vectors[pl.ds(0, 1), :], partner_vectors[pl.ds(0, 1), :])
    projected = jnp.dot(token_all[...], weight_in[...], preferred_element_type=jnp.float32)
    projected = projected.astype(jnp.bfloat16)
    pool_rows[...] = projected[:, :width]
    query, forget_logit, value = (
        projected[:, n * width : (n + 1) * width].astype(jnp.float32) for n in range(1, 4)
    )
    spike_row = lax.broadcasted_iota(jnp.int32, (8, width), 0)
    wanted_row = jnp.logical_or(spike_row == column, spike_row == column + 4)
    spike_columns = []
    for n in range(4):
        parts = spikes[2 * n + half].astype(jnp.float32)
        line = jnp.sum(jnp.where(wanted_row, parts, 0.0), axis=0, keepdims=True)
        spike_columns.append(jnp.broadcast_to(line, (width, width)).T)
    spike = jnp.concatenate(spike_columns, axis=0)
    reader = query * jax.nn.sigmoid(query)
    key_gate = jax.nn.sigmoid(-lower_bound) * jax.nn.sigmoid(-forget_logit)
    log_decay = jnp.log1p(-key_gate) + spike
    t_at = lax.broadcasted_iota(jnp.int32, (BLOCK, BLOCK), 0)
    s_at = lax.broadcasted_iota(jnp.int32, (BLOCK, BLOCK), 1)
    causal = t_at >= s_at
    lower = causal.astype(jnp.float32)
    length = 4 * rows_each
    states = [jnp.zeros((width, width), jnp.float32)] * 2
    before = [jnp.zeros((1, width), jnp.float32)] * 2
    for n in range(length // BLOCK):
        for seq in range(2):
            begin = seq * length + n * BLOCK
            rows = slice(begin, begin + BLOCK)
            inner_log = jnp.dot(
                lower, log_decay[rows], preferred_element_type=jnp.float32, precision=HIGHEST
            )
            keys = key_gate[rows]
            values = value[rows].astype(jnp.bfloat16)
            grown = reader[rows] * jnp.exp(inner_log)
            read_scaled = grown.astype(jnp.bfloat16)
            key_scaled = (keys * jnp.exp(-inner_log)).astype(jnp.bfloat16)
            scores = lax.dot_general(
                read_scaled, key_scaled, (((1,), (1,)), ((), ())), preferred_element_type=jnp.float32
            )
            scores = jnp.where(causal, scores, 0.0).astype(jnp.bfloat16)
            read = jnp.dot(scores, values, preferred_element_type=jnp.float32)
            if n > 0:
                read = read + jnp.dot(
                    read_scaled,
                    states[seq].astype(jnp.bfloat16),
                    preferred_element_type=jnp.float32,
                )
            closing = inner_log[BLOCK - 1 : BLOCK]
            key_tail = (keys * jnp.exp(closing - inner_log)).astype(jnp.bfloat16)
            added = lax.dot_general(
                key_tail, values, (((0,), (0,)), ((), ())), preferred_element_type=jnp.float32
            )
            share = jnp.broadcast_to(jnp.exp(closing), (width, width)).T
            states[seq] = share * states[seq] + added
            read_local[pl.ds(begin, BLOCK), :] = read
            read_full[pl.ds(begin, BLOCK), :] = (grown * jnp.exp(before[seq])).astype(jnp.bfloat16)
            before[seq] = before[seq] + closing
    for seq in range(2):
        top = seq * (width + HALO)
        carry[pl.ds(top, width), :] = states[seq].astype(jnp.bfloat16)
        carry[pl.ds(top + width, HALO), :] = projected[
            (seq + 1) * length - HALO : (seq + 1) * length, :width
        ]


def output_kernel(width, rows_each, *refs):
    own_vectors, partner_vectors, read_local, read_full, pool_rows, carry = refs[:6]
    pieces, blocks = refs[6:14], refs[14:16]
    sent, kept = refs[16:18]
    weight_out, mixed, sems = refs[18:]
    plane, late, half, row, side, core = places()
    owns = core == half
    plane_rows = 4 * width
    part = plane_rows // 2
    length = 4 * rows_each

    def put(source, n):
        x = side if n == 0 else 1 - side
        return weight_out.at[source, :, pl.ds(pl.multiple_of(x * part, part), part)]

    ends = [[(block.at[pl.ds(plane_rows, 2 * width), :], weight_out.at[plane])] for block in blocks]
    pairs = [pieces[2 * n : 2 * n + 2] for n in range(4)]
    waits = start_pieces(pairs, ends, sems, plane, core, owns, put)
    head_gain = jnp.where(owns, own_vectors[pl.ds(1, 1), :], partner_vectors[pl.ds(1, 1), :])
    group = 2 * half + row
    window = jnp.left_shift(jnp.int32(2), group)
    for seq in range(2):
        top = seq * (width + HALO)
        rows = pl.ds(seq * length, length)
        extended = jnp.concatenate(
            [carry[pl.ds(top + width, HALO), :], pool_rows[rows, :]], axis=0
        ).astype(jnp.float32)
        window_sum = extended
        chosen = jnp.zeros_like(extended)
        for g in range(4):
            window_sum = window_sum + down(window_sum, 2**g)
            chosen = jnp.where(group == g, window_sum, chosen)
        at = lax.broadcasted_iota(jnp.int32, (length, width), 0) + late * length
        counts = jnp.minimum(at + 1, window).astype(jnp.float32)
        mixed[rows, pl.ds(0, width)] = (chosen[HALO:] / counts - extended[HALO:]).astype(
            jnp.bfloat16
        )
        read = read_local[rows, :] + jnp.dot(
            read_full[rows, :], carry[pl.ds(top, width), :], preferred_element_type=jnp.float32
        )
        mixed[rows, pl.ds(width, width)] = (rms_scale(read, 1.0) * head_gain).astype(jnp.bfloat16)
    for copy in waits:
        copy.wait()
    for target, c in ((sent, 1 - core), (kept, core)):
        for n in range(4):
            top = pl.multiple_of((n * 2 + c) * rows_each, rows_each)
            rows = mixed[pl.ds(top, rows_each), :]
            for p in range(weight_out.shape[0]):
                target[n // 2, n % 2, :, pl.ds(p * plane_rows, plane_rows)] = jnp.dot(
                    rows, weight_out[p], preferred_element_type=jnp.float32
                ).astype(jnp.bfloat16)


def join_kernel(*refs):
    kept, received, left_send, right_send, left_keep, right_keep = refs
    _, _, half, row, _, _ = places()
    middle = kept.shape[-1] // 2
    left, right = pl.ds(0, middle), pl.ds(middle, middle)
    for n in range(2):
        for target, at in (
            (left_send, (1 - row, n, slice(None), left)),
            (right_send, (n, 1 - half, slice(None), right)),
            (left_keep, (row, n, slice(None), left)),
            (right_keep, (n, half, slice(None), right)),
        ):
            total = kept[at].astype(jnp.float32) + received[at].astype(jnp.float32)
            target[n] = total.astype(target.dtype)


def by_halves(
    tokens,
    input_norm_gain,
    pooling_input_weight,
    query_weight,
    forget_weight,
    value_weight,
    pooling_group_maps,
    pooling_scale,
    lower_bound_logits,
    decay_spike,
    head_norm_gain,
    pooling_output_weight,
    recurrent_output_weight,
):
    planes, members, cores = (lax.axis_size(axis) for axis in ("sp", "fs", "tp"))
    _, _, half, row, _, _ = places()
    heads = decay_spike.shape[2]
    width = query_weight.shape[1] // heads
    features = tokens.shape[2]
    rows_each = tokens.shape[1]
    part = query_weight.shape[0] // 2
    hbm = pl.BlockSpec(memory_space=pltpu.HBM)
    vmem = pl.BlockSpec(memory_space=pltpu.VMEM)

    def made(*shape, kind=jnp.bfloat16):
        return pltpu.VMEM(shape, kind)

    def near(*values):
        return [pltpu.with_memory_space_constraint(v, pltpu.VMEM) for v in values]

    def pack(*refs):
        pack_kernel(width, *refs)

    def far(*values):
        return [pltpu.with_memory_space_constraint(v, pltpu.HBM) for v in values]

    weights_in = far(pooling_input_weight, query_weight, forget_weight, value_weight)

    def first(*refs):
        first_kernel(width, rows_each, *refs)

    *messages, own_rows = pl.pallas_call(
        first,
        out_shape=[made(part, 4 * width)] * 2 + [made(rows_each + 8, features)],
        in_specs=[hbm] * 7,
        out_specs=[vmem] * 3,
        scratch_shapes=[
            pltpu.VMEM((rows_each, features), jnp.bfloat16),
            pltpu.VMEM((1, features), jnp.float32),
            pltpu.VMEM((heads, width), jnp.float32),
            pltpu.SemaphoreType.DMA((11,)),
        ],
        compiler_params=pltpu.CompilerParams(vmem_limit_bytes=8 * MEBI),
        name="first",
    )(*far(tokens[0], input_norm_gain[None], decay_spike[0].T), *weights_in)
    *out_messages, partner_block, own_block, vectors, partner_vectors, _ = pl.pallas_call(
        pack,
        out_shape=[made(2 * width, part)] * 2
        + [made(2 * part + 2 * width, 4 * width)] * 2
        + [made(2, width, kind=jnp.float32)] * 2
        + [made(2 * width, 4 * width)],
        in_specs=[hbm] * 10,
        out_specs=[vmem] * 7,
        scratch_shapes=[
            pltpu.VMEM(pooling_group_maps.shape[1:], jnp.bfloat16),
            pltpu.VMEM((2 * width, 4 * width), jnp.bfloat16),
        ]
        + [pltpu.VMEM((1, heads * width), jnp.float32)] * 3
        + [
            pltpu.SemaphoreType.DMA((17,)),
        ],
        compiler_params=pltpu.CompilerParams(vmem_limit_bytes=12 * MEBI),
        name="pack",
    )(
        *far(pooling_scale[None], lower_bound_logits[None], head_norm_gain[None]),
        *weights_in,
        *far(pooling_group_maps, pooling_output_weight, recurrent_output_weight),
    )

    def hops(wanted):
        return [
            (((p + k) % planes) * cores + p % cores, p * cores + c)
            for p in range(planes)
            for k, c in wanted
        ]

    rounds = (
        (0, hops([(2, 0), (1, 1)])),
        (1, hops([(2, 1), (1, 0)])),
        (1, hops([(3, 0)])),
        (0, hops([(3, 1)])),
    )

    def shared(pair):
        pieces = []
        for n, (which, pairs) in enumerate(rounds):
            arrived = lax.ppermute(pair[which], ("sp", "tp"), pairs)
            pieces.append(arrived)
            used = range(cores) if n < 2 else (n - 2,)
            across = [(f * cores + c, (f ^ 1) * cores + c) for f in range(members) for c in used]
            pieces.append(lax.ppermute(arrived, ("fs", "tp"), across))
        return pieces

    pieces = shared(messages)
    output_pieces = shared(out_messages)
    partner_local = swapped(partner_block, "tp", 1)

    received_vectors = swapped(partner_vectors, "tp", 1)
    other_rows = swapped(own_rows, "sp", 1)
    chip_rows = []
    for rows in (own_rows, other_rows):
        chip_rows += [rows, swapped(rows, "fs", 2)]
    token_pieces = []
    for rows in chip_rows:
        token_pieces += [rows, swapped(rows, "tp", 1)]

    length = 8 * rows_each
    carry_shape = made(2 * (width + HALO), width)

    def state(*refs):
        state_kernel(width, rows_each, *refs)

    read_local, read_full, pool_rows, carry = pl.pallas_call(
        state,
        out_shape=[
            made(length, width, kind=jnp.float32),
            made(length, width),
            made(length, width),
            carry_shape,
        ],
        in_specs=[vmem] * 20,
        out_specs=[vmem] * 4,
        scratch_shapes=[
            pltpu.VMEM((length, features), jnp.bfloat16),
            pltpu.VMEM((features, 4 * width), jnp.bfloat16),
            pltpu.VMEM((8, 8, width), jnp.bfloat16),
            pltpu.SemaphoreType.DMA((16,)),
            pltpu.SemaphoreType.DMA((7,)),
        ],
        compiler_params=pltpu.CompilerParams(vmem_limit_bytes=24 * MEBI),
        name="state",
    )(
        *near(vectors, received_vectors, *token_pieces, *pieces, own_block, partner_local),
    )
    entering_carry = lax.ppermute(carry, "sp", [(p, p + 2) for p in range(planes - 2)])

    def output(*refs):
        output_kernel(width, rows_each, *refs)

    half_shape = made(2, 2, rows_each, features)
    sent, kept = pl.pallas_call(
        output,
        out_shape=[half_shape] * 2,
        in_specs=[vmem] * 16,
        out_specs=[vmem] * 2,
        scratch_shapes=[
            pltpu.VMEM((planes, 2 * width, 4 * width), jnp.bfloat16),
            pltpu.VMEM((length, 2 * width), jnp.bfloat16),
            pltpu.SemaphoreType.DMA((7,)),
        ],
        compiler_params=pltpu.CompilerParams(vmem_limit_bytes=20 * MEBI),
        name="output",
    )(
        *near(vectors, received_vectors, read_local, read_full, pool_rows, entering_carry),
        *near(*output_pieces, own_block, partner_local),
    )
    from_partner = swapped(sent, "tp", 1)
    middle = features // 2

    portion = (2, rows_each, middle)
    left_send, right_send, left_keep, right_keep = pl.pallas_call(
        join_kernel,
        out_shape=[made(*portion)] * 2 + [made(*portion, kind=jnp.float32)] * 2,
        in_specs=[vmem] * 2,
        out_specs=[vmem] * 4,
        compiler_params=pltpu.CompilerParams(vmem_limit_bytes=12 * MEBI),
        name="join",
    )(*near(kept, from_partner))
    left_in = swapped(left_send, "fs", 2)
    right_in = swapped(right_send, "sp", 1)
    left_sum = left_keep + left_in.astype(jnp.float32)
    right_sum = right_keep + right_in.astype(jnp.float32)
    left_last = swapped(picked(left_sum, 1 - half).astype(jnp.bfloat16), "sp", 1)
    right_last = swapped(picked(right_sum, 1 - row).astype(jnp.bfloat16), "fs", 2)
    left_total = picked(left_sum, half) + left_last.astype(jnp.float32)
    right_total = picked(right_sum, row) + right_last.astype(jnp.float32)
    total = jnp.concatenate([left_total, right_total], axis=1)
    return total.astype(jnp.bfloat16)[None]


def body(*arrays):
    tokens, _, pool_in, query_in, _, _, maps, _, _, spike, _, pool_out, _ = arrays
    if halves_divide(tokens, query_in, pool_in, maps, spike, pool_out):
        return by_halves(*arrays)
    return by_positions(*arrays)


def by_positions(
    tokens,
    input_norm_gain,
    pooling_input_weight,
    query_weight,
    forget_weight,
    value_weight,
    pooling_group_maps,
    pooling_scale,
    lower_bound_logits,
    decay_spike,
    head_norm_gain,
    pooling_output_weight,
    recurrent_output_weight,
):
    gathered = lax.all_gather(tokens, "tp", axis=1, tiled=True)[0]
    length_total = gathered.shape[0]
    normed = rms_scale(gathered.astype(jnp.float32), input_norm_gain).astype(jnp.bfloat16)
    pool_width = pooling_input_weight.shape[1]
    rec_width = query_weight.shape[1]
    stacked = jnp.concatenate(
        [pooling_input_weight, query_weight, forget_weight, value_weight], axis=1
    )
    out_local = jnp.concatenate([pooling_output_weight, recurrent_output_weight], axis=0)
    groups_fs = lax.axis_size("fs")
    member = lax.axis_index("fs")
    slice_width = stacked.shape[1] // groups_fs
    own_slice = lax.dynamic_slice_in_dim(stacked, member * slice_width, slice_width, 1)
    column_part = lax.all_gather(own_slice, "sp", axis=0, tiled=True)
    full_input = lax.all_gather(column_part, "fs", axis=1, tiled=True)
    projected = jnp.dot(normed, full_input, preferred_element_type=jnp.float32)
    slice_height = out_local.shape[0] // groups_fs
    own_rows = lax.dynamic_slice_in_dim(out_local, member * slice_height, slice_height, 0)
    row_part = lax.all_gather(own_rows, "sp", axis=1, tiled=True)
    out_full = lax.all_gather(row_part, "fs", axis=0, tiled=True)
    rounded = lax.optimization_barrier(projected.astype(jnp.bfloat16))
    pool_input = rounded[:, :pool_width]
    query_matrix = rounded[:, pool_width : pool_width + rec_width].astype(jnp.float32)
    forget_gate_logit = rounded[:, pool_width + rec_width : pool_width + 2 * rec_width].astype(
        jnp.float32
    )
    value_projected = rounded[:, pool_width + 2 * rec_width :].astype(jnp.float32)
    groups_local = pooling_group_maps.shape[0]
    group_size = pooling_group_maps.shape[1]
    reach_rows = 2 ** (groups_local * lax.axis_size("tp"))
    previous = shifted(pool_input[length_total - reach_rows :], "sp", 1)
    extended = jnp.concatenate([previous, pool_input], axis=0).astype(jnp.float32)
    extended = extended.reshape(reach_rows + length_total, groups_local, group_size)
    group_ids = lax.axis_index("tp") * groups_local + jnp.arange(groups_local, dtype=jnp.int32)
    windows = jnp.left_shift(jnp.int32(2), group_ids)
    window_sum = jnp.zeros((length_total, groups_local, group_size), jnp.float32)
    for offset in range(reach_rows):
        inside = (offset < windows).astype(jnp.float32)
        window_sum = (
            window_sum
            + extended[reach_rows - offset : reach_rows - offset + length_total] * inside[:, None]
        )
    position_index = lax.axis_index("sp") * length_total + jnp.arange(length_total, dtype=jnp.int32)
    counts = jnp.minimum(position_index[:, None] + 1, windows[None, :]).astype(jnp.float32)
    pool_diff = (window_sum / counts[:, :, None] - extended[reach_rows:]).astype(jnp.bfloat16)
    pool_mapped = jnp.einsum(
        "tgc,gcd->tgd", pool_diff, pooling_group_maps, preferred_element_type=jnp.float32
    )
    pool_out = (pool_mapped.reshape(length_total, pool_width) * pooling_scale).astype(jnp.bfloat16)
    local_heads = decay_spike.shape[2]
    head_width = rec_width // local_heads
    blocks = length_total // BLOCK
    block_layout = (blocks, BLOCK, local_heads, head_width)
    reader = jax.nn.silu(query_matrix).reshape(block_layout)
    key_gate_value = jax.nn.sigmoid(-lower_bound_logits) * jax.nn.sigmoid(-forget_gate_logit)
    decay_logarithm = (
        jnp.log1p(-key_gate_value).reshape(length_total, local_heads, head_width)
        + decay_spike[0][:, :, None]
    ).reshape(block_layout)
    key_rows = key_gate_value.reshape(block_layout)
    value_rows = value_projected.reshape(block_layout)
    inner_log = jnp.cumsum(decay_logarithm, axis=1)
    read_scaled = reader * jnp.exp(inner_log)
    key_scaled = key_rows * jnp.exp(-inner_log)
    causal = (jnp.arange(BLOCK)[:, None] >= jnp.arange(BLOCK)[None, :]).astype(jnp.float32)
    scores = jnp.einsum("nthd,nshd->nhts", read_scaled, key_scaled, precision=HIGHEST) * causal
    within = jnp.einsum("nhts,nshe->nthe", scores, value_rows, precision=HIGHEST)
    closing = inner_log[:, -1]
    key_tail = key_rows * jnp.exp(closing[:, None] - inner_log)
    deltas = jnp.einsum("nshd,nshe->nhde", key_tail, value_rows, precision=HIGHEST)
    block_decay = jnp.exp(closing)

    def advance(carried, input_batch):
        decay_now, delta_now = input_batch
        return (decay_now[..., None] * carried + delta_now, carried)

    initial = jnp.zeros((local_heads, head_width, head_width), jnp.float32)
    device_state, entry_states = lax.scan(advance, initial, (block_decay, deltas))
    device_decay = jnp.exp(jnp.sum(closing, axis=0))
    scanned = entering(
        (device_decay, device_state),
        "sp",
        join_state,
        (jnp.ones_like(device_decay), jnp.zeros_like(device_state)),
    )
    prior_state = scanned[1]
    before = jnp.cumsum(closing, axis=0) - closing
    start_states = entry_states + jnp.exp(before)[..., None] * prior_state[None]
    read_out = within + jnp.einsum("nthd,nhde->nthe", read_scaled, start_states, precision=HIGHEST)
    read_out = read_out.reshape(length_total, local_heads, head_width)
    recurrent_output = (
        rms_scale(read_out, 1.0).reshape(length_total, rec_width) * head_norm_gain
    ).astype(jnp.bfloat16)
    mixed_rows = jnp.concatenate([pool_out, recurrent_output], axis=1)
    summed = lax.psum_scatter(
        jnp.dot(mixed_rows, out_full, preferred_element_type=jnp.float32).astype(jnp.bfloat16),
        "tp",
        scatter_dimension=0,
        tiled=True,
    )
    return summed[None]


def solution(mesh):
    placed = (
        P("fs", ("sp", "tp"), None),
        P(),
        P("sp", "tp"),
        P("sp", "tp"),
        P("sp", "tp"),
        P("sp", "tp"),
        P("tp", None, None),
        P("tp"),
        P("tp"),
        P("fs", "sp", "tp"),
        P("tp"),
        P("tp", "sp"),
        P("tp", "sp"),
    )
    return jax.shard_map(
        body, mesh=mesh, in_specs=placed, out_specs=P("fs", ("sp", "tp"), None), check_vma=False
    )
```

```python
import jax
import jax.numpy as jnp
from jax import lax
from jax.experimental import pallas as pl
from jax.experimental.pallas import tpu as pltpu
from jax.sharding import PartitionSpec as P

BLOCK = 64


EPSILON = 1e-06
HIGHEST = lax.Precision.HIGHEST


def shifted(value, axis, steps):
    count = lax.axis_size(axis)
    first, last = (max(0, -steps), min(count, count - steps))
    return lax.ppermute(value, axis, [(source, source + steps) for source in range(first, last)])


def entering(shard, axis, join, neutral):
    place = lax.axis_index(axis)
    gathered = jax.tree.map(
        lambda a, kind: lax.all_gather(a.astype(kind), axis), shard, (jnp.bfloat16, jnp.bfloat16)
    )
    state = jax.tree.map(lambda a, e: jnp.zeros_like(a) + jnp.asarray(e, a.dtype), shard, neutral)

    def one(step, state):
        return join(
            state,
            jax.tree.map(
                lambda a, own: lax.dynamic_index_in_dim(a, step, 0, False).astype(own.dtype),
                gathered,
                shard,
            ),
        )

    return lax.fori_loop(0, place, one, state)


def rms_scale(values, gain):
    return values * lax.rsqrt(jnp.mean(values * values, axis=-1, keepdims=True) + EPSILON) * gain


def join_state(earlier, later):
    decay_one, state_one = earlier
    decay_two, state_two = later
    return (decay_one * decay_two, decay_two[..., None] * state_one + state_two)


def swapped(value, axis, bits):
    count = lax.axis_size(axis)
    return lax.ppermute(value, axis, [(source, source ^ bits) for source in range(count)])


def halves_divide(tokens, query_weight, pooling_input_weight, pooling_group_maps, decay_spike, out_weight):
    planes, members, cores = (lax.axis_size(axis) for axis in ("sp", "fs", "tp"))
    heads = decay_spike.shape[2]
    width = query_weight.shape[1] // heads
    return (
        cores == 2
        and planes == 2 * cores
        and members == 2 * cores
        and heads == 2 * cores
        and width % 128 == 0
        and pooling_group_maps.shape[0] * 2 == heads
        and pooling_input_weight.shape[1] == query_weight.shape[1]
        and tokens.shape[0] == 1
        and tokens.shape[1] % BLOCK == 0
        and decay_spike.shape[1] == cores * tokens.shape[1] == width
        and query_weight.shape[0] == heads * width
        and out_weight.shape[1] == heads * width
        and pooling_group_maps.shape[1] == 2 * width
        and 2 ** (2 * pooling_group_maps.shape[0]) <= HALO
    )


HALO = 16
MEBI = 2**20


def places():
    plane, member, core = (lax.axis_index(axis) for axis in ("sp", "fs", "tp"))
    late, half = lax.div(plane, 2), lax.rem(plane, 2)
    row, side = lax.div(member, 2), lax.rem(member, 2)
    return plane, late, half, row, side, core


def first_kernel(width, rows_each, *refs):
    sources, inputs, messages, rows_out = refs[:3], refs[3:7], refs[7:9], refs[9]
    locals_in, sems = refs[10:13], refs[13]
    tokens, gain, spikes = locals_in
    _, _, half, row, side, core = places()
    loads = [
        pltpu.make_async_copy(source, target, sems.at[8 + n])
        for n, (source, target) in enumerate(zip(sources, locals_in))
    ]
    for copy in loads:
        copy.start()
    part = inputs[0].shape[0] // 2
    top = pl.multiple_of(side * part, part)
    first = jnp.where(core == half, 0, 1)
    copies = []
    for n in range(2):
        place = 2 * row + jnp.where(n == 0, first, 1 - first)
        column = pl.multiple_of(place * width, width)
        for m, w in enumerate(inputs):
            copies.append(
                pltpu.make_async_copy(
                    w.at[pl.ds(top, part), pl.ds(column, width)],
                    messages[n].at[:, pl.ds(m * width, width)],
                    sems.at[n * 4 + m],
                )
            )
    for copy in copies:
        copy.start()
    for copy in loads:
        copy.wait()
    values = tokens[...].astype(jnp.float32)
    rows_out[pl.ds(0, rows_each), :] = rms_scale(values, gain[...]).astype(jnp.bfloat16)
    rows_out[pl.ds(rows_each, 8), :] = jnp.zeros((8, rows_out.shape[1]), jnp.bfloat16)
    upper = spikes[...].astype(jnp.bfloat16)
    lower = (spikes[...] - upper.astype(jnp.float32)).astype(jnp.bfloat16)
    rows_out[pl.ds(rows_each, 8), pl.ds(0, width)] = jnp.concatenate([upper, lower], axis=0)
    for copy in copies:
        copy.wait()


def pack_kernel(width, *refs):
    sources = refs[:3]
    inputs, maps, pool_weight, rec_weight = refs[3:7], refs[7], refs[8], refs[9]
    messages, blocks, own_vectors, partner_vectors, pooled = refs[10:12], refs[12:14], *refs[14:17]
    group_map, group_rows, scale, bound, head_gain, sems = refs[17:]
    _, _, half, row, side, core = places()
    rows = inputs[0].shape[0]
    size = maps.shape[1]
    begin = pl.multiple_of(row * size, size)
    first = jnp.where(core == half, 0, 1)
    group_copies = [
        pltpu.make_async_copy(maps.at[row], group_map, sems.at[0]),
        pltpu.make_async_copy(pool_weight.at[pl.ds(begin, size), :], group_rows, sems.at[1]),
    ]
    group_copies += [
        pltpu.make_async_copy(source, target, sems.at[14 + n])
        for n, (source, target) in enumerate(zip(sources, (scale, bound, head_gain)))
    ]
    copies = []
    targets = []
    top = pl.ds(pl.multiple_of(side * (rows // 2), rows // 2), rows // 2)
    for n, place in enumerate((1 - core, core)):
        column = pl.multiple_of((2 * row + place) * width, width)
        copies += [
            pltpu.make_async_copy(
                w.at[:, pl.ds(column, width)],
                blocks[n].at[pl.ds(0, rows), pl.ds(m * width, width)],
                sems.at[2 + 4 * n + m],
            )
            for m, w in enumerate(inputs)
        ]
        targets.append((place, slice(None), blocks[n].at[pl.ds(rows + width, width), :]))
    for n in range(2):
        place = jnp.where(n == 0, first, 1 - first)
        targets.append((place, top, messages[n].at[pl.ds(width, width), :]))
    for n, (place, columns, target) in enumerate(targets):
        at = pl.ds(pl.multiple_of((2 * row + place) * width, width), width)
        copies.append(pltpu.make_async_copy(rec_weight.at[at, columns], target, sems.at[10 + n]))
    for copy in group_copies + copies:
        copy.start()
    for copy in group_copies:
        copy.wait()
    for place, target in ((2 * row + core, own_vectors), (2 * row + 1 - core, partner_vectors)):
        at = pl.ds(pl.multiple_of(place * width, width), width)
        for n, vector in enumerate((bound, head_gain)):
            target[pl.ds(n, 1), :] = vector[:, at]
    scaled = group_map[...].astype(jnp.float32) * scale[:, pl.ds(begin, size)]
    high = scaled.astype(jnp.bfloat16)
    rest = (scaled - high.astype(jnp.float32)).astype(jnp.bfloat16)
    pooled[...] = (
        jnp.dot(high, group_rows[...], preferred_element_type=jnp.float32)
        + jnp.dot(rest, group_rows[...], preferred_element_type=jnp.float32)
    ).astype(jnp.bfloat16)
    for block, place in zip(blocks, (1 - core, core)):
        block[pl.ds(rows, width), :] = pooled[pl.ds(pl.multiple_of(place * width, width), width), :]
    for n in range(2):
        place = jnp.where(n == 0, first, 1 - first)
        messages[n][pl.ds(0, width), :] = pooled[
            pl.ds(pl.multiple_of(place * width, width), width), top
        ]
    for copy in copies:
        copy.wait()


def down(values, steps):
    rows = lax.broadcasted_iota(jnp.int32, values.shape, 0)
    return jnp.where(rows >= steps, pltpu.roll(values, steps, 0), 0.0)


def start_pieces(pieces, blocks, sems, plane, core, owns, put):
    planes = lax.axis_size("sp")
    near, far, last = (
        lax.rem(plane + k, planes) for k in (2 - core, 1 + core, 3)
    )
    waits = []
    used = 0

    def copies(group, source, slot):
        return [
            pltpu.make_async_copy(piece, put(source, n), sems.at[slot + n])
            for n, piece in enumerate(group)
        ]

    for group, source in zip(pieces[:2], (near, far)):
        made = copies(group, source, used)
        for copy in made:
            copy.start()
        waits += made
        used += len(group)
    choices = [copies(group, last, used) for group in pieces[2:]]
    for n in range(2):

        @pl.when(core == n)
        def _(n=n):
            for copy in choices[n]:
                copy.start()

    waits += choices[0]
    used += len(choices[0])
    for n, group in enumerate(blocks):
        for m, (source, target) in enumerate(group):
            copy = pltpu.make_async_copy(source, target, sems.at[used + m])

            @pl.when(owns if n == 0 else jnp.logical_not(owns))
            def _(copy=copy):
                copy.start()

            if n == 0:
                waits.append(copy)
    return waits


def state_kernel(width, rows_each, *refs):
    own_vectors, partner_vectors = refs[:2]
    tokens, pieces, blocks = refs[2:10], refs[10:18], refs[18:20]
    read_local, read_full, pool_rows, carry = refs[20:24]
    token_all, weight_in, spikes, token_sems, sems = refs[24:]
    plane, _, half, row, side, core = places()
    owns = core == half
    column = 2 * row + core
    plane_rows = 4 * width
    part = plane_rows // 2
    waits = []
    used = 0
    for a in range(2):
        for b in range(2):
            for c in range(2):
                piece = tokens[(a * 2 + b) * 2 + c]
                order = ((row ^ b) * 2 + (half ^ a)) * 2 + (core ^ c)
                top = pl.multiple_of(order * rows_each, rows_each)
                waits.append(
                    pltpu.make_async_copy(
                        piece.at[pl.ds(0, rows_each), :],
                        token_all.at[pl.ds(top, rows_each), :],
                        token_sems.at[used],
                    )
                )
                waits.append(
                    pltpu.make_async_copy(
                        piece.at[pl.ds(rows_each, 8), pl.ds(0, width)],
                        spikes.at[order],
                        token_sems.at[used + 1],
                    )
                )
                used += 2
    for copy in waits:
        copy.start()

    def put(source, n):
        x = side if n == 0 else 1 - side
        return weight_in.at[pl.ds(pl.multiple_of(source * plane_rows + x * part, part), part), :]

    begin = pl.ds(pl.multiple_of(plane * plane_rows, plane_rows), plane_rows)
    ends = [[(block.at[pl.ds(0, plane_rows), :], weight_in.at[begin, :])] for block in blocks]
    pairs = [pieces[2 * n : 2 * n + 2] for n in range(4)]
    more = start_pieces(pairs, ends, sems, plane, core, owns, put)
    for copy in waits + more:
        copy.wait()
    lower_bound = jnp.where(owns, own_vectors[pl.ds(0, 1), :], partner_vectors[pl.ds(0, 1), :])
    projected = jnp.dot(token_all[...], weight_in[...], preferred_element_type=jnp.float32)
    projected = projected.astype(jnp.bfloat16)
    pool_rows[...] = projected[:, :width]
    query, forget_logit, value = (
        projected[:, n * width : (n + 1) * width].astype(jnp.float32) for n in range(1, 4)
    )
    spike_row = lax.broadcasted_iota(jnp.int32, (8, width), 0)
    wanted_row = jnp.logical_or(spike_row == column, spike_row == column + 4)
    spike_columns = []
    for n in range(4):
        parts = spikes[2 * n + half].astype(jnp.float32)
        line = jnp.sum(jnp.where(wanted_row, parts, 0.0), axis=0, keepdims=True)
        spike_columns.append(jnp.broadcast_to(line, (width, width)).T)
    spike = jnp.concatenate(spike_columns, axis=0)
    reader = query * jax.nn.sigmoid(query)
    key_gate = jax.nn.sigmoid(-lower_bound) * jax.nn.sigmoid(-forget_logit)
    log_decay = jnp.log1p(-key_gate) + spike
    t_at = lax.broadcasted_iota(jnp.int32, (BLOCK, BLOCK), 0)
    s_at = lax.broadcasted_iota(jnp.int32, (BLOCK, BLOCK), 1)
    causal = t_at >= s_at
    lower = causal.astype(jnp.float32)
    length = 4 * rows_each
    states = [jnp.zeros((width, width), jnp.float32)] * 2
    before = [jnp.zeros((1, width), jnp.float32)] * 2
    for n in range(length // BLOCK):
        for seq in range(2):
            begin = seq * length + n * BLOCK
            rows = slice(begin, begin + BLOCK)
            inner_log = jnp.dot(
                lower, log_decay[rows], preferred_element_type=jnp.float32, precision=HIGHEST
            )
            keys = key_gate[rows]
            values = value[rows].astype(jnp.bfloat16)
            grown = reader[rows] * jnp.exp(inner_log)
            read_scaled = grown.astype(jnp.bfloat16)
            key_scaled = (keys * jnp.exp(-inner_log)).astype(jnp.bfloat16)
            scores = lax.dot_general(
                read_scaled, key_scaled, (((1,), (1,)), ((), ())), preferred_element_type=jnp.float32
            )
            scores = jnp.where(causal, scores, 0.0).astype(jnp.bfloat16)
            read = jnp.dot(scores, values, preferred_element_type=jnp.float32)
            if n > 0:
                read = read + jnp.dot(
                    read_scaled,
                    states[seq].astype(jnp.bfloat16),
                    preferred_element_type=jnp.float32,
                )
            closing = inner_log[BLOCK - 1 : BLOCK]
            key_tail = (keys * jnp.exp(closing - inner_log)).astype(jnp.bfloat16)
            added = lax.dot_general(
                key_tail, values, (((0,), (0,)), ((), ())), preferred_element_type=jnp.float32
            )
            share = jnp.broadcast_to(jnp.exp(closing), (width, width)).T
            states[seq] = share * states[seq] + added
            read_local[pl.ds(begin, BLOCK), :] = read
            read_full[pl.ds(begin, BLOCK), :] = (grown * jnp.exp(before[seq])).astype(jnp.bfloat16)
            before[seq] = before[seq] + closing
    for seq in range(2):
        top = seq * (width + HALO)
        carry[pl.ds(top, width), :] = states[seq].astype(jnp.bfloat16)
        carry[pl.ds(top + width, HALO), :] = projected[
            (seq + 1) * length - HALO : (seq + 1) * length, :width
        ]


def output_kernel(width, rows_each, *refs):
    own_vectors, partner_vectors, read_local, read_full, pool_rows, carry = refs[:6]
    pieces, blocks = refs[6:14], refs[14:16]
    sent, kept = refs[16:18]
    weight_out, mixed, sems = refs[18:]
    plane, late, half, row, side, core = places()
    owns = core == half
    plane_rows = 4 * width
    part = plane_rows // 2
    length = 4 * rows_each

    def put(source, n):
        x = side if n == 0 else 1 - side
        return weight_out.at[source, :, pl.ds(pl.multiple_of(x * part, part), part)]

    ends = [[(block.at[pl.ds(plane_rows, 2 * width), :], weight_out.at[plane])] for block in blocks]
    pairs = [pieces[2 * n : 2 * n + 2] for n in range(4)]
    waits = start_pieces(pairs, ends, sems, plane, core, owns, put)
    head_gain = jnp.where(owns, own_vectors[pl.ds(1, 1), :], partner_vectors[pl.ds(1, 1), :])
    group = 2 * half + row
    window = jnp.left_shift(jnp.int32(2), group)
    for seq in range(2):
        top = seq * (width + HALO)
        rows = pl.ds(seq * length, length)
        extended = jnp.concatenate(
            [carry[pl.ds(top + width, HALO), :], pool_rows[rows, :]], axis=0
        ).astype(jnp.float32)
        window_sum = extended
        chosen = jnp.zeros_like(extended)
        for g in range(4):
            window_sum = window_sum + down(window_sum, 2**g)
            chosen = jnp.where(group == g, window_sum, chosen)
        at = lax.broadcasted_iota(jnp.int32, (length, width), 0) + late * length
        counts = jnp.minimum(at + 1, window).astype(jnp.float32)
        mixed[rows, pl.ds(0, width)] = (chosen[HALO:] / counts - extended[HALO:]).astype(
            jnp.bfloat16
        )
        read = read_local[rows, :] + jnp.dot(
            read_full[rows, :], carry[pl.ds(top, width), :], preferred_element_type=jnp.float32
        )
        mixed[rows, pl.ds(width, width)] = (rms_scale(read, 1.0) * head_gain).astype(jnp.bfloat16)
    for copy in waits:
        copy.wait()
    for target, c in ((sent, 1 - core), (kept, core)):
        for n in range(4):
            top = pl.multiple_of((n * 2 + c) * rows_each, rows_each)
            rows = mixed[pl.ds(top, rows_each), :]
            for p in range(weight_out.shape[0]):
                target[n // 2, n % 2, :, pl.ds(p * plane_rows, plane_rows)] = jnp.dot(
                    rows, weight_out[p], preferred_element_type=jnp.float32
                ).astype(jnp.bfloat16)


def join_kernel(*refs):
    kept, received = refs[:2]
    _, _, half, row, _, _ = places()
    ends = ((1 - row, 1 - half), (1 - row, half), (row, 1 - half), (row, half))
    for target, at in zip(refs[2:], ends):
        total = kept[at].astype(jnp.float32) + received[at].astype(jnp.float32)
        target[...] = total.astype(target.dtype)


def by_halves(
    tokens,
    input_norm_gain,
    pooling_input_weight,
    query_weight,
    forget_weight,
    value_weight,
    pooling_group_maps,
    pooling_scale,
    lower_bound_logits,
    decay_spike,
    head_norm_gain,
    pooling_output_weight,
    recurrent_output_weight,
):
    planes, members, cores = (lax.axis_size(axis) for axis in ("sp", "fs", "tp"))
    plane, late, half, row, side, core = places()
    heads = decay_spike.shape[2]
    width = query_weight.shape[1] // heads
    features = tokens.shape[2]
    rows_each = tokens.shape[1]
    part = query_weight.shape[0] // 2
    hbm = pl.BlockSpec(memory_space=pltpu.HBM)
    vmem = pl.BlockSpec(memory_space=pltpu.VMEM)

    def made(*shape, kind=jnp.bfloat16):
        return pltpu.VMEM(shape, kind)

    def near(*values):
        return [pltpu.with_memory_space_constraint(v, pltpu.VMEM) for v in values]

    def pack(*refs):
        pack_kernel(width, *refs)

    def far(*values):
        return [pltpu.with_memory_space_constraint(v, pltpu.HBM) for v in values]

    weights_in = far(pooling_input_weight, query_weight, forget_weight, value_weight)

    def first(*refs):
        first_kernel(width, rows_each, *refs)

    *messages, own_rows = pl.pallas_call(
        first,
        out_shape=[made(part, 4 * width)] * 2 + [made(rows_each + 8, features)],
        in_specs=[hbm] * 7,
        out_specs=[vmem] * 3,
        scratch_shapes=[
            pltpu.VMEM((rows_each, features), jnp.bfloat16),
            pltpu.VMEM((1, features), jnp.float32),
            pltpu.VMEM((heads, width), jnp.float32),
            pltpu.SemaphoreType.DMA((11,)),
        ],
        compiler_params=pltpu.CompilerParams(vmem_limit_bytes=8 * MEBI),
        name="first",
    )(*far(tokens[0], input_norm_gain[None], decay_spike[0].T), *weights_in)
    *out_messages, partner_block, own_block, vectors, partner_vectors, _ = pl.pallas_call(
        pack,
        out_shape=[made(2 * width, part)] * 2
        + [made(2 * part + 2 * width, 4 * width)] * 2
        + [made(2, width, kind=jnp.float32)] * 2
        + [made(2 * width, 4 * width)],
        in_specs=[hbm] * 10,
        out_specs=[vmem] * 7,
        scratch_shapes=[
            pltpu.VMEM(pooling_group_maps.shape[1:], jnp.bfloat16),
            pltpu.VMEM((2 * width, 4 * width), jnp.bfloat16),
        ]
        + [pltpu.VMEM((1, heads * width), jnp.float32)] * 3
        + [
            pltpu.SemaphoreType.DMA((17,)),
        ],
        compiler_params=pltpu.CompilerParams(vmem_limit_bytes=12 * MEBI),
        name="pack",
    )(
        *far(pooling_scale[None], lower_bound_logits[None], head_norm_gain[None]),
        *weights_in,
        *far(pooling_group_maps, pooling_output_weight, recurrent_output_weight),
    )

    def hops(wanted):
        return [
            (((p + k) % planes) * cores + p % cores, p * cores + c)
            for p in range(planes)
            for k, c in wanted
        ]

    rounds = (
        (0, hops([(2, 0), (1, 1)])),
        (1, hops([(2, 1), (1, 0)])),
        (1, hops([(3, 0)])),
        (0, hops([(3, 1)])),
    )

    def shared(pair):
        pieces = []
        for n, (which, pairs) in enumerate(rounds):
            arrived = lax.ppermute(pair[which], ("sp", "tp"), pairs)
            pieces.append(arrived)
            used = range(cores) if n < 2 else (n - 2,)
            across = [(f * cores + c, (f ^ 1) * cores + c) for f in range(members) for c in used]
            pieces.append(lax.ppermute(arrived, ("fs", "tp"), across))
        return pieces

    pieces = shared(messages)
    output_pieces = shared(out_messages)
    partner_local = swapped(partner_block, "tp", 1)

    received_vectors = swapped(partner_vectors, "tp", 1)
    other_rows = swapped(own_rows, "sp", 1)
    chip_rows = []
    for rows in (own_rows, other_rows):
        chip_rows += [rows, swapped(rows, "fs", 2)]
    token_pieces = []
    for rows in chip_rows:
        token_pieces += [rows, swapped(rows, "tp", 1)]

    length = 8 * rows_each
    carry_shape = made(2 * (width + HALO), width)

    def state(*refs):
        state_kernel(width, rows_each, *refs)

    read_local, read_full, pool_rows, carry = pl.pallas_call(
        state,
        out_shape=[
            made(length, width, kind=jnp.float32),
            made(length, width),
            made(length, width),
            carry_shape,
        ],
        in_specs=[vmem] * 20,
        out_specs=[vmem] * 4,
        scratch_shapes=[
            pltpu.VMEM((length, features), jnp.bfloat16),
            pltpu.VMEM((features, 4 * width), jnp.bfloat16),
            pltpu.VMEM((8, 8, width), jnp.bfloat16),
            pltpu.SemaphoreType.DMA((16,)),
            pltpu.SemaphoreType.DMA((7,)),
        ],
        compiler_params=pltpu.CompilerParams(vmem_limit_bytes=24 * MEBI),
        name="state",
    )(
        *near(vectors, received_vectors, *token_pieces, *pieces, own_block, partner_local),
    )
    entering_carry = lax.ppermute(carry, "sp", [(p, p + 2) for p in range(planes - 2)])

    def output(*refs):
        output_kernel(width, rows_each, *refs)

    half_shape = made(2, 2, rows_each, features)
    sent, kept = pl.pallas_call(
        output,
        out_shape=[half_shape] * 2,
        in_specs=[vmem] * 16,
        out_specs=[vmem] * 2,
        scratch_shapes=[
            pltpu.VMEM((planes, 2 * width, 4 * width), jnp.bfloat16),
            pltpu.VMEM((length, 2 * width), jnp.bfloat16),
            pltpu.SemaphoreType.DMA((7,)),
        ],
        compiler_params=pltpu.CompilerParams(vmem_limit_bytes=20 * MEBI),
        name="output",
    )(
        *near(vectors, received_vectors, read_local, read_full, pool_rows, entering_carry),
        *near(*output_pieces, own_block, partner_local),
    )
    from_partner = swapped(sent, "tp", 1)
    portion = (rows_each, features)
    across_send, row_send, plane_send, kept_rows = pl.pallas_call(
        join_kernel,
        out_shape=[made(*portion)] * 3 + [made(*portion, kind=jnp.float32)],
        in_specs=[vmem] * 2,
        out_specs=[vmem] * 4,
        compiler_params=pltpu.CompilerParams(vmem_limit_bytes=12 * MEBI),
        name="join",
    )(*near(kept, from_partner))
    corners = [
        (p * members + f, (p ^ 1) * members + (f ^ 2)) for p in range(planes) for f in range(members)
    ]
    across = lax.ppermute(across_send, ("sp", "fs"), corners)
    from_row = swapped(row_send, "fs", 2)
    from_plane = swapped(plane_send, "sp", 1)
    total = kept_rows + across.astype(jnp.float32) + from_row.astype(jnp.float32)
    total = total + from_plane.astype(jnp.float32)
    return total.astype(jnp.bfloat16)[None]


def body(*arrays):
    tokens, _, pool_in, query_in, _, _, maps, _, _, spike, _, pool_out, _ = arrays
    if halves_divide(tokens, query_in, pool_in, maps, spike, pool_out):
        return by_halves(*arrays)
    return by_positions(*arrays)


def by_positions(
    tokens,
    input_norm_gain,
    pooling_input_weight,
    query_weight,
    forget_weight,
    value_weight,
    pooling_group_maps,
    pooling_scale,
    lower_bound_logits,
    decay_spike,
    head_norm_gain,
    pooling_output_weight,
    recurrent_output_weight,
):
    gathered = lax.all_gather(tokens, "tp", axis=1, tiled=True)[0]
    length_total = gathered.shape[0]
    normed = rms_scale(gathered.astype(jnp.float32), input_norm_gain).astype(jnp.bfloat16)
    pool_width = pooling_input_weight.shape[1]
    rec_width = query_weight.shape[1]
    stacked = jnp.concatenate(
        [pooling_input_weight, query_weight, forget_weight, value_weight], axis=1
    )
    out_local = jnp.concatenate([pooling_output_weight, recurrent_output_weight], axis=0)
    groups_fs = lax.axis_size("fs")
    member = lax.axis_index("fs")
    slice_width = stacked.shape[1] // groups_fs
    own_slice = lax.dynamic_slice_in_dim(stacked, member * slice_width, slice_width, 1)
    column_part = lax.all_gather(own_slice, "sp", axis=0, tiled=True)
    full_input = lax.all_gather(column_part, "fs", axis=1, tiled=True)
    projected = jnp.dot(normed, full_input, preferred_element_type=jnp.float32)
    slice_height = out_local.shape[0] // groups_fs
    own_rows = lax.dynamic_slice_in_dim(out_local, member * slice_height, slice_height, 0)
    row_part = lax.all_gather(own_rows, "sp", axis=1, tiled=True)
    out_full = lax.all_gather(row_part, "fs", axis=0, tiled=True)
    rounded = lax.optimization_barrier(projected.astype(jnp.bfloat16))
    pool_input = rounded[:, :pool_width]
    query_matrix = rounded[:, pool_width : pool_width + rec_width].astype(jnp.float32)
    forget_gate_logit = rounded[:, pool_width + rec_width : pool_width + 2 * rec_width].astype(
        jnp.float32
    )
    value_projected = rounded[:, pool_width + 2 * rec_width :].astype(jnp.float32)
    groups_local = pooling_group_maps.shape[0]
    group_size = pooling_group_maps.shape[1]
    reach_rows = 2 ** (groups_local * lax.axis_size("tp"))
    previous = shifted(pool_input[length_total - reach_rows :], "sp", 1)
    extended = jnp.concatenate([previous, pool_input], axis=0).astype(jnp.float32)
    extended = extended.reshape(reach_rows + length_total, groups_local, group_size)
    group_ids = lax.axis_index("tp") * groups_local + jnp.arange(groups_local, dtype=jnp.int32)
    windows = jnp.left_shift(jnp.int32(2), group_ids)
    window_sum = jnp.zeros((length_total, groups_local, group_size), jnp.float32)
    for offset in range(reach_rows):
        inside = (offset < windows).astype(jnp.float32)
        window_sum = (
            window_sum
            + extended[reach_rows - offset : reach_rows - offset + length_total] * inside[:, None]
        )
    position_index = lax.axis_index("sp") * length_total + jnp.arange(length_total, dtype=jnp.int32)
    counts = jnp.minimum(position_index[:, None] + 1, windows[None, :]).astype(jnp.float32)
    pool_diff = (window_sum / counts[:, :, None] - extended[reach_rows:]).astype(jnp.bfloat16)
    pool_mapped = jnp.einsum(
        "tgc,gcd->tgd", pool_diff, pooling_group_maps, preferred_element_type=jnp.float32
    )
    pool_out = (pool_mapped.reshape(length_total, pool_width) * pooling_scale).astype(jnp.bfloat16)
    local_heads = decay_spike.shape[2]
    head_width = rec_width // local_heads
    blocks = length_total // BLOCK
    block_layout = (blocks, BLOCK, local_heads, head_width)
    reader = jax.nn.silu(query_matrix).reshape(block_layout)
    key_gate_value = jax.nn.sigmoid(-lower_bound_logits) * jax.nn.sigmoid(-forget_gate_logit)
    decay_logarithm = (
        jnp.log1p(-key_gate_value).reshape(length_total, local_heads, head_width)
        + decay_spike[0][:, :, None]
    ).reshape(block_layout)
    key_rows = key_gate_value.reshape(block_layout)
    value_rows = value_projected.reshape(block_layout)
    inner_log = jnp.cumsum(decay_logarithm, axis=1)
    read_scaled = reader * jnp.exp(inner_log)
    key_scaled = key_rows * jnp.exp(-inner_log)
    causal = (jnp.arange(BLOCK)[:, None] >= jnp.arange(BLOCK)[None, :]).astype(jnp.float32)
    scores = jnp.einsum("nthd,nshd->nhts", read_scaled, key_scaled, precision=HIGHEST) * causal
    within = jnp.einsum("nhts,nshe->nthe", scores, value_rows, precision=HIGHEST)
    closing = inner_log[:, -1]
    key_tail = key_rows * jnp.exp(closing[:, None] - inner_log)
    deltas = jnp.einsum("nshd,nshe->nhde", key_tail, value_rows, precision=HIGHEST)
    block_decay = jnp.exp(closing)

    def advance(carried, input_batch):
        decay_now, delta_now = input_batch
        return (decay_now[..., None] * carried + delta_now, carried)

    initial = jnp.zeros((local_heads, head_width, head_width), jnp.float32)
    device_state, entry_states = lax.scan(advance, initial, (block_decay, deltas))
    device_decay = jnp.exp(jnp.sum(closing, axis=0))
    scanned = entering(
        (device_decay, device_state),
        "sp",
        join_state,
        (jnp.ones_like(device_decay), jnp.zeros_like(device_state)),
    )
    prior_state = scanned[1]
    before = jnp.cumsum(closing, axis=0) - closing
    start_states = entry_states + jnp.exp(before)[..., None] * prior_state[None]
    read_out = within + jnp.einsum("nthd,nhde->nthe", read_scaled, start_states, precision=HIGHEST)
    read_out = read_out.reshape(length_total, local_heads, head_width)
    recurrent_output = (
        rms_scale(read_out, 1.0).reshape(length_total, rec_width) * head_norm_gain
    ).astype(jnp.bfloat16)
    mixed_rows = jnp.concatenate([pool_out, recurrent_output], axis=1)
    summed = lax.psum_scatter(
        jnp.dot(mixed_rows, out_full, preferred_element_type=jnp.float32).astype(jnp.bfloat16),
        "tp",
        scatter_dimension=0,
        tiled=True,
    )
    return summed[None]


def solution(mesh):
    placed = (
        P("fs", ("sp", "tp"), None),
        P(),
        P("sp", "tp"),
        P("sp", "tp"),
        P("sp", "tp"),
        P("sp", "tp"),
        P("tp", None, None),
        P("tp"),
        P("tp"),
        P("fs", "sp", "tp"),
        P("tp"),
        P("tp", "sp"),
        P("tp", "sp"),
    )
    return jax.shard_map(
        body, mesh=mesh, in_specs=placed, out_specs=P("fs", ("sp", "tp"), None), check_vma=False
    )
```
